32 devices in a mesh: kv: 8 (over z, y), tp: 4 (over x, core).
Axes of the slice: x: 2, y: 2, z: 4, core: 2. Of those that a mesh axis runs over, the one named last changes fastest.
Arguments:
- tokens: bfloat16 [32, 4096], P(None, 'kv'), may hold values from -40 to 40, as said below
- norm_gain: float32 [4096], P('kv'), may hold values from 0.1 to 1.9
- w_query: bfloat16 [4096, 2048], P('kv', 'tp'), may hold values from -0.09375 to 0.09375
- w_key: bfloat16 [4096, 512], P('kv', 'tp'), may hold values from -0.09375 to 0.09375
- w_value: bfloat16 [4096, 512], P('kv', 'tp'), may hold values from -0.09375 to 0.09375
- forget_weight: bfloat16 [4096, 32], replicated, may hold values from -0.09375 to 0.09375
- forget_bias: float32 [32], P('tp'), may hold values from -1 to 3
- kv_cache: bfloat16 [32, 10240, 8, 128], P(None, 'kv', 'tp'), may hold values from -6 to 6
- cum_gates: float32 [32, 32, 10240], P(None, 'tp', 'kv'), may hold values from -10500 to 0, as said below
- lengths: int32 [32], replicated, may hold values from 1 to 10240, as said below
- w_out: bfloat16 [2048, 4096], P('tp', 'kv'), may hold values from -0.25 to 0.25
Outputs:
- mixed: bfloat16 [32, 4096], P(None, 'kv')
- log_weight: float32 [32, 32], P(None, 'tp')
The draws below stay inside these ranges and needn't reach their ends.
Inputs may be any that keep to these rules, and one draw needn't show every extreme that they name: Columns of tokens come in 16 groups of equal width. `cum_gates`: each row does not rise along the positions. `lengths`: some sequence has all 10240 positions cached.
All inputs are finite; a program needn't handle non-finite values.
Results may differ from the reference program's by a relative error of at most 0.0307.
Values may be sent and summed in bfloat16 or wider, within the bound.
A program may use at most 128 MiB of HBM per device.

```python
import math
import jax
import jax.numpy as jnp
from jax import lax

D = 4096
HEADS = 32
KV_HEADS = 8
HEAD = 64
BATCH = 32
CTX_DEV = 1280
LENGTH = 10240
N_KV = 8
N_TP = 4


def draw_tokens(key, part):
    first_key, second_key, third_key = jax.random.split(key, 3)
    base = jax.random.normal(first_key, (BATCH, D), jnp.float32)
    group_scale = jnp.exp(jax.random.uniform(second_key, (16,), jnp.float32, math.log(0.3), math.log(3.0)))
    columns = jnp.repeat(group_scale, D // 16)
    values = base * columns
    return jnp.clip(values, -40.0, 40.0).astype(jnp.bfloat16)


def draw_cum_gates(key, part):
    first_key, second_key, third_key = jax.random.split(key, 3)
    shift_key = jax.random.fold_in(key, 11)
    pick_key, depth_key, forced_key = jax.random.split(shift_key, 3)
    fast_share = 0.5
    is_fast = jax.random.uniform(first_key, (BATCH, HEADS), jnp.float32) < fast_share
    rate = jnp.where(is_fast, 1.0 / 30.0, 1.0 / LENGTH)
    block_factor = jnp.exp(jax.random.uniform(second_key, (BATCH, HEADS, LENGTH // CTX_DEV), jnp.float32, math.log(0.35), math.log(2.8)))
    block_factor = jnp.repeat(block_factor, CTX_DEV, axis=2)
    step_size = jax.random.uniform(third_key, (BATCH, HEADS, LENGTH), jnp.float32, 0.2, 1.8)
    log_forget = -rate[:, :, None] * block_factor * step_size
    shifted = jax.random.uniform(pick_key, (BATCH, HEADS), jnp.float32) < 0.25
    depth = jax.random.uniform(depth_key, (BATCH, HEADS), jnp.float32, 120.0, 260.0)
    forced = jax.random.randint(forced_key, (), 0, BATCH * HEADS)
    flat_index = jnp.arange(BATCH * HEADS, dtype=jnp.int32).reshape(BATCH, HEADS)
    offset = jnp.where(shifted, -depth, 0.0)
    offset = jnp.where(flat_index == forced, -jnp.maximum(depth, 200.0), offset)
    return jnp.cumsum(log_forget, axis=2) + offset[:, :, None]


def draw_lengths(key, part):
    first_key, second_key = jax.random.split(key)
    values = jax.random.randint(first_key, (BATCH,), 1, LENGTH + 1).astype(jnp.int32)
    chosen = jax.random.randint(second_key, (), 0, BATCH)
    return values.at[chosen].set(LENGTH).astype(jnp.int32)


def level_of(key, shape, cuts, low, largest):
    gain = 1.0
    for axis_at, blocks in cuts:
        draws = jax.random.uniform(jax.random.fold_in(jax.random.fold_in(key, 6), axis_at), (blocks,), jnp.float32, low / len(cuts), largest / len(cuts))
        gain = gain * jnp.repeat(jnp.exp(draws), shape[axis_at] // blocks).reshape((-1,) + (1,) * (len(shape) - 1 - axis_at))
    return gain


def noise(rng, dims, scale, most, cuts=(), kind=jnp.bfloat16):
    entries = jax.random.normal(rng, dims, jnp.float32) * scale
    if len(cuts) > 0:
        entries = level_of(rng, dims, cuts, -0.22, 0.18) * entries
    return jnp.clip(entries, min=-most, max=most).astype(kind)


def setup_inputs(seed: int = 0) -> dict:
    key_list = jax.random.split(jax.random.key(seed), 12)
    tokens = draw_tokens(jax.random.fold_in(key_list[11], 71), 0)
    norm_gain = jnp.clip(1.0 + 0.18 * jax.random.normal(key_list[1], (D,), jnp.float32), 0.1, 1.9)
    w_query = noise(key_list[2], (D, HEADS * HEAD), D ** -0.5, 0.09375, ((0, 8), (1, 4)))
    w_key = noise(key_list[3], (D, KV_HEADS * HEAD), D ** -0.5, 0.09375, ((0, 8), (1, 4)))
    w_value = noise(key_list[4], (D, KV_HEADS * HEAD), D ** -0.5, 0.09375, ((0, 8), (1, 4)))
    forget_weight = noise(key_list[5], (D, HEADS), D ** -0.5, 0.09375)
    forget_bias = jnp.clip(-1.0 + 4.0 * jax.random.uniform(key_list[6], (HEADS,), jnp.float32) ** level_of(key_list[6], (HEADS,), ((0, 4),), -0.2, 0.2), -1.0, 3.0)
    kv_cache = noise(key_list[7], (BATCH, LENGTH, KV_HEADS, 2 * HEAD), 1.0, 6.0, ((1, 8), (2, 4)))
    cum_gates = draw_cum_gates(jax.random.fold_in(key_list[11], 71), 0)
    lengths = draw_lengths(jax.random.fold_in(key_list[11], 71), 0)
    w_out = noise(key_list[10], (HEADS * HEAD, D), (HEAD * 8) ** -0.5, 0.25, ((0, 4), (1, 8)))
    return dict(tokens=tokens, norm_gain=norm_gain, w_query=w_query, w_key=w_key, w_value=w_value, forget_weight=forget_weight, forget_bias=forget_bias, kv_cache=kv_cache, cum_gates=cum_gates, lengths=lengths, w_out=w_out)


norm_eps = 1e-05
masked_floor = -1e+30

def reference(tokens, norm_gain, w_query, w_key, w_value, forget_weight, forget_bias, kv_cache, cum_gates, lengths, w_out):
    tokens_f = tokens.astype(jnp.float32)
    row_scale = lax.rsqrt(lax.optimization_barrier(jnp.mean(tokens_f * tokens_f, axis=1)) + norm_eps)[:, None]
    normalized_input = (tokens_f * norm_gain).astype(jnp.bfloat16)
    query = (row_scale * jnp.dot(normalized_input, w_query, preferred_element_type=jnp.float32)).astype(jnp.bfloat16)
    fresh_key_row = (row_scale * jnp.dot(normalized_input, w_key, preferred_element_type=jnp.float32)).astype(jnp.bfloat16)
    value_new = (row_scale * jnp.dot(normalized_input, w_value, preferred_element_type=jnp.float32)).astype(jnp.bfloat16)
    log_gate = jax.nn.log_sigmoid(row_scale * jnp.dot(normalized_input, forget_weight, preferred_element_type=jnp.float32) + forget_bias)
    group_size = HEADS // KV_HEADS
    inv_root = HEAD ** (-0.5)

    def one_row(items):
        query_row, key_row, value_row, forget_gate_row, cache_row, cum_row, length = items
        query_head_rows = query_row.astype(jnp.float32).reshape(KV_HEADS, group_size, HEAD)
        cached_keys = cache_row[:, :, :HEAD].astype(jnp.float32)
        cached_vals = cache_row[:, :, HEAD:].astype(jnp.float32)
        scores = jnp.einsum('kgd,lkd->kgl', query_head_rows, cached_keys) * inv_root
        biased = scores - cum_row.reshape(KV_HEADS, group_size, LENGTH)
        last_cum = lax.dynamic_index_in_dim(cum_row, (length - 1).astype(jnp.int32), axis=1, keepdims=False)
        cum_query = last_cum + forget_gate_row
        key_heads = key_row.astype(jnp.float32).reshape(KV_HEADS, HEAD)
        new_biased = jnp.einsum('kgd,kd->kg', query_head_rows, key_heads) * inv_root - cum_query.reshape(KV_HEADS, group_size)
        blocked = biased.reshape(KV_HEADS, group_size, N_KV, CTX_DEV)
        in_range = (jnp.arange(LENGTH, dtype=jnp.int32) < length).reshape(N_KV, CTX_DEV)
        holds_last = jnp.arange(N_KV, dtype=jnp.int32) == (length - 1) // CTX_DEV
        block_peak = lax.optimization_barrier(jnp.max(jnp.where(in_range, blocked, masked_floor), axis=-1))
        block_peak = jnp.where(holds_last, jnp.maximum(block_peak, new_biased[..., None]), block_peak)
        weights = jnp.where(in_range, jnp.exp(blocked - block_peak[..., None]), 0.0)
        new_weight = jnp.where(holds_last, jnp.exp(new_biased[..., None] - block_peak), 0.0)
        block_sum = lax.optimization_barrier(jnp.sum(weights, axis=-1)) + new_weight
        rounded = lax.optimization_barrier(weights.astype(jnp.bfloat16)).astype(jnp.float32)
        rounded_new = lax.optimization_barrier(new_weight.astype(jnp.bfloat16)).astype(jnp.float32)
        value_block_rows = jnp.einsum('kgnl,nlkd->kgnd', rounded, cached_vals.reshape(N_KV, CTX_DEV, KV_HEADS, HEAD))
        value_heads = value_row.astype(jnp.float32).reshape(KV_HEADS, 1, 1, HEAD)
        value_block_rows = value_block_rows + rounded_new[..., None] * value_heads
        peak = lax.optimization_barrier(jnp.max(block_peak, axis=-1))
        rescale_factor = jnp.exp(block_peak - peak[..., None])
        weight_sum = lax.optimization_barrier(jnp.sum(block_sum * rescale_factor, axis=-1))
        values = lax.optimization_barrier(jnp.sum(value_block_rows * rescale_factor[..., None], axis=2))
        attended = (values / weight_sum[..., None]).astype(jnp.bfloat16).reshape(HEADS * HEAD)
        log_weight = (peak + jnp.log(weight_sum)).reshape(HEADS) + cum_query
        return (attended, log_weight)
    attended, log_weight = lax.map(one_row, (query, fresh_key_row, value_new, log_gate, kv_cache, cum_gates, lengths))
    group_cols = HEADS * HEAD // N_TP
    pieces = attended.astype(jnp.float32).reshape(BATCH, N_TP, group_cols)
    out_rows = w_out.astype(jnp.float32).reshape(N_TP, group_cols, D)
    partial_out = jnp.einsum('bgc,gcd->gbd', pieces, out_rows).astype(jnp.bfloat16)
    partial_out = lax.optimization_barrier(partial_out)
    mixed = lax.optimization_barrier(jnp.sum(partial_out.astype(jnp.float32), axis=0)).astype(jnp.bfloat16)
    return (mixed, log_weight)
```

```python
import functools
import jax
import jax.numpy as jnp
from jax import lax
from jax.experimental import pallas as pl
from jax.experimental.pallas import tpu as pltpu
from jax.sharding import PartitionSpec as P

norm_eps = 1e-05
masked_floor = -1e30
LANES = 128
MESH = pl.DeviceIdType.MESH


def flip(index, step, count):
    out = index
    bit = 1
    while bit < count:
        out = out + bit * ((step // bit) % 2) * (1 - 2 * ((index // bit) % 2))
        bit *= 2
    return out


def lane_of(shape):
    return lax.broadcasted_iota(jnp.int32, shape, len(shape) - 1)


def kernel(
    n_kv,
    n_tp,
    tokens_ref,
    gain_ref,
    bias_ref,
    lengths_ref,
    w_query_hbm,
    w_key_hbm,
    w_value_hbm,
    gate_hbm,
    cache_hbm,
    cum_hbm,
    w_out_hbm,
    mixed_ref,
    log_ref,
    w_query_ref,
    w_key_ref,
    w_value_ref,
    gate_ref,
    cache_ref,
    cum_ref,
    w_out_ref,
    shift_ref,
    last_ref,
    proj_ref,
    rs1_ref,
    query_ref,
    new_ref,
    bias_pad_ref,
    wide_ref,
    score_ref,
    peak_ref,
    value_ref,
    stat_ref,
    part_ref,
    gathered_ref,
    fresh_ref,
    order_ref,
    wide_rows_ref,
    tp_ref,
    weight_sems,
    cache_sems,
    rs1_send,
    rs1_recv,
    ag1_send,
    ag1_recv,
    new_send,
    new_recv,
    part_send,
    part_recv,
    tp_send,
    tp_recv,
):
    f32, bf16 = jnp.float32, jnp.bfloat16
    me = lax.axis_index("kv")
    my_tp = lax.axis_index("tp")
    rows, cols = tokens_ref.shape
    heads = cum_ref.shape[1]
    span = cum_ref.shape[2]
    entries = cache_ref.shape[1]
    kv_local = entries // span
    group = heads // kv_local
    head_size = LANES // 2
    all_heads = gate_hbm.shape[0]
    mine = rows // n_kv
    pairs = mine // 2
    tall = mine * heads
    q_cols = w_query_ref.shape[1]
    k_cols = w_key_ref.shape[1]
    k_pad = -(-k_cols // LANES) * LANES
    model_width = cols * n_kv
    inv_root = head_size ** (-0.5)
    chunk_cols = 2 * LANES
    chunks = range(0, entries, chunk_cols)
    segment = LANES // 4

    gate_ref[...] = jnp.zeros_like(gate_ref)
    offset = pl.multiple_of(me * cols, cols)
    loads = [
        pltpu.make_async_copy(src, dst, weight_sems.at[i])
        for i, (src, dst) in enumerate(
            [
                (w_query_hbm, w_query_ref),
                (w_key_hbm, w_key_ref),
                (w_value_hbm, w_value_ref),
                (gate_hbm.at[:, pl.ds(offset, cols)], gate_ref.at[pl.ds(0, all_heads)]),
                (cum_hbm, cum_ref),
                (w_out_hbm, w_out_ref),
            ]
        )
    ]
    for load in loads[:5]:
        load.start()

    def cache_load(owner):
        at = pl.ds(owner * mine, mine)
        return pltpu.make_async_copy(cache_hbm.at[at], cache_ref.at[at], cache_sems.at[owner])

    barrier = pltpu.get_barrier_semaphore()
    for step in range(1, n_kv):
        pl.semaphore_signal(
            barrier, inc=1, device_id={"kv": flip(me, step, n_kv)}, device_id_type=MESH
        )
    for step in range(1, n_tp):
        pl.semaphore_signal(
            barrier, inc=1, device_id={"tp": flip(my_tp, step, n_tp)}, device_id_type=MESH
        )

    tokens_f = tokens_ref[...].astype(f32)
    squares = jnp.sum(tokens_f * tokens_f, axis=1, keepdims=True)
    normed = (tokens_f * gain_ref[...]).astype(bf16)
    bias_pad_ref[...] = jnp.zeros_like(bias_pad_ref)
    bias_pad_ref[:, 0:heads] = bias_ref[...]
    for load in loads[:4]:
        load.wait()
    for step in range(n_kv):
        cache_load(flip(me, step, n_kv)).start()
    loads[5].start()
    pieces = [jnp.dot(normed, w_query_ref[...], preferred_element_type=f32)]
    for w_ref in (w_key_ref, w_value_ref):
        piece = jnp.dot(normed, w_ref[...], preferred_element_type=f32)
        if k_pad > k_cols:
            piece = jnp.concatenate([piece, jnp.zeros((rows, k_pad - k_cols), f32)], axis=1)
        pieces.append(piece)
    gates = lax.dot_general(
        normed, gate_ref[...], (((1,), (1,)), ((), ())), preferred_element_type=f32
    )
    pieces.append(jnp.where(lane_of(gates.shape) == all_heads, squares, gates))
    at = 0
    for piece in pieces:
        for owner in range(n_kv):
            proj_ref[owner, :, at : at + piece.shape[1]] = piece[
                owner * mine : (owner + 1) * mine
            ].astype(bf16)
        at += piece.shape[1]

    def rs1_copy(source, target):
        return pltpu.make_async_remote_copy(
            src_ref=proj_ref.at[target],
            dst_ref=rs1_ref.at[source],
            send_sem=rs1_send.at[target],
            recv_sem=rs1_recv.at[source],
            device_id={"kv": target},
            device_id_type=MESH,
        )

    pl.semaphore_wait(barrier, n_kv + n_tp - 2)
    for step in reversed(range(1, n_kv)):
        rs1_copy(me, flip(me, step, n_kv)).start()

    loads[4].wait()
    tile = (heads, LANES)
    lane = lane_of(tile)
    own_column = (lane % kv_local) == (lax.broadcasted_iota(jnp.int32, tile, 0) // group)

    def prepare(row, carry):
        length = lengths_ref[row] - me * span
        last = jnp.zeros(tile, f32)
        for chunk in range(span // LANES):
            cum = cum_ref[row, :, chunk * LANES : (chunk + 1) * LANES]
            place = lane + chunk * LANES
            shift = jnp.where(place < length, -cum, masked_floor)
            last = last + jnp.where(place == length - 1, cum, 0.0)
            for part in range(kv_local):
                if kv_local == 1:
                    spread = shift
                else:
                    pick = lane // kv_local + part * (LANES // kv_local)
                    spread = jnp.take_along_axis(shift, pick, axis=1)
                    spread = jnp.where(own_column, spread, masked_floor)
                at = (chunk * kv_local + part) * LANES
                shift_ref[row, :, at : at + LANES] = spread
        last_ref[row] = jnp.broadcast_to(jnp.sum(last, axis=1, keepdims=True), tile)
        return carry

    lax.fori_loop(0, rows, prepare, 0, unroll=4)

    piece_rows = LANES
    narrow = lane_of((piece_rows, LANES)) < head_size

    def pack(owner):
        cache_load(owner).wait()

        def body(i, carry):
            inside = pl.ds(pl.multiple_of(i * piece_rows, piece_rows), piece_rows)
            for pair in range(pairs):
                row = owner * mine + 2 * pair
                first, second = cache_ref[row, inside, :], cache_ref[row + 1, inside, :]
                turned = pltpu.roll(second, head_size, 1)
                cache_ref[row, inside, :] = jnp.where(narrow, first, turned)
                cache_ref[row + 1, inside, :] = jnp.where(narrow, turned, first)
            return carry

        lax.fori_loop(0, entries // piece_rows, body, 0, unroll=2)

    def pack_step(step, carry):
        pack(flip(me, step, n_kv))
        return carry

    lax.fori_loop(0, n_kv, pack_step, 0)

    total = proj_ref[me].astype(f32)
    for step in range(1, n_kv):
        other = flip(me, step, n_kv)
        rs1_copy(other, me).wait_recv()
        total = total + rs1_ref[other].astype(f32)
    misc = total[:, q_cols + 2 * k_pad :]
    part_lane = lane_of((mine, LANES))
    total_sq = jnp.sum(jnp.where(part_lane == all_heads, misc, 0.0), axis=1, keepdims=True)
    row_scale = lax.rsqrt(total_sq / model_width + norm_eps)
    query_ref[me] = (row_scale * total[:, :q_cols]).astype(bf16)

    def ag1_copy(source, target):
        return pltpu.make_async_remote_copy(
            src_ref=query_ref.at[source],
            dst_ref=query_ref.at[source],
            send_sem=ag1_send.at[target],
            recv_sem=ag1_recv.at[source],
            device_id={"kv": target},
            device_id_type=MESH,
        )

    for step in reversed(range(1, n_kv)):
        ag1_copy(me, flip(me, step, n_kv)).start()

    low_half = part_lane < head_size
    even_row = lax.broadcasted_iota(jnp.int32, (mine, LANES), 0) % 2 == 0

    def grouped(values, width):
        tiles = []
        for at in range(0, width, LANES):
            halves = []
            for half in range(2):
                source = (at // head_size + half) // group
                found = values[:, (source // 2) * LANES : (source // 2 + 1) * LANES]
                if source % 2 != half:
                    found = pltpu.roll(found, head_size, 1)
                halves.append(found)
            low = lane_of(halves[0].shape) < head_size
            tiles.append(jnp.where(low, halves[0], halves[1]))
        return jnp.concatenate(tiles, axis=1)

    head_shape = (LANES, q_cols)
    head_map = (
        lax.broadcasted_iota(jnp.int32, head_shape, 0) % heads
        == lax.broadcasted_iota(jnp.int32, head_shape, 1) // head_size
    ).astype(f32).astype(bf16)

    new_key = (row_scale * total[:, q_cols : q_cols + k_pad]).astype(bf16).astype(f32)
    new_value = (row_scale * total[:, q_cols + k_pad : q_cols + 2 * k_pad]).astype(bf16)
    product = query_ref[me].astype(f32) * grouped(new_key, q_cols)
    coarse = product.astype(bf16)
    fine = (product - coarse.astype(f32)).astype(bf16)
    new_score = sum(
        lax.dot_general(part, head_map, (((1,), (1,)), ((), ())), preferred_element_type=f32)
        for part in (coarse, fine)
    )
    gate = pltpu.roll(row_scale * misc, (LANES - my_tp * heads) % LANES, 1) + bias_pad_ref[...]
    log_gate = jnp.minimum(gate, 0.0) - jnp.log1p(jnp.exp(-jnp.abs(gate)))
    new_ref[me, :, :k_pad] = new_value.astype(f32)
    new_ref[me, :, k_pad:] = jnp.where(
        part_lane < heads, new_score * inv_root, pltpu.roll(log_gate, heads, 1)
    )

    def new_copy(source, target):
        return pltpu.make_async_remote_copy(
            src_ref=new_ref.at[source],
            dst_ref=new_ref.at[source],
            send_sem=new_send.at[target],
            recv_sem=new_recv.at[source],
            device_id={"kv": target},
            device_id_type=MESH,
        )

    for step in reversed(range(1, n_kv)):
        new_copy(me, flip(me, step, n_kv)).start()

    def part_copy(source, block, target):
        return pltpu.make_async_remote_copy(
            src_ref=part_ref.at[source, block],
            dst_ref=part_ref.at[source, block],
            send_sem=part_send.at[block, target],
            recv_sem=part_recv.at[block, source],
            device_id={"kv": target},
            device_id_type=MESH,
        )

    tall_row = lax.broadcasted_iota(jnp.int32, (tall, LANES), 0)
    tall_lane = lane_of((tall, LANES))
    stat_kind = (tall_lane % segment) // heads

    def spread(owner):
        query = query_ref[owner].astype(f32) * inv_root
        for at in range(0, q_cols, LANES):
            straight = query[:, at : at + LANES]
            turned = pltpu.roll(straight, head_size, 1)
            for half in range(2):
                low, high = (straight, turned) if half == 0 else (turned, straight)
                head = at // head_size + half
                wide_ref[pl.ds(head, mine, stride=heads), :] = jnp.where(
                    even_row, jnp.where(low_half, low, 0.0), jnp.where(low_half, 0.0, high)
                )
        wide = wide_ref[...]
        return jnp.concatenate(
            [
                jnp.where(tall_row // (2 * heads) == pair, wide, 0.0)
                for pair in range(pairs)
            ],
            axis=1,
        ).astype(bf16)

    def packed(owner, side, at):
        inside = slice(at, at + chunk_cols)
        return jnp.concatenate(
            [cache_ref[owner * mine + 2 * pair + side, inside, :] for pair in range(pairs)],
            axis=1,
        )

    def score(owner, queries, at):
        part = lax.dot_general(
            queries,
            packed(owner, 0, at),
            (((1,), (1,)), ((), ())),
            preferred_element_type=f32,
        )
        part = part + jnp.concatenate(
            [shift_ref[owner * mine + i, :, at : at + chunk_cols] for i in range(mine)], axis=0
        )
        score_ref[:, at : at + chunk_cols] = part
        return part

    def weigh(owner, peak, sums, values, at):
        weight = jnp.exp(score_ref[:, at : at + chunk_cols] - peak)
        values = values + jnp.dot(
            weight.astype(bf16), packed(owner, 1, at), preferred_element_type=f32
        )
        return sums + weight, values

    def set_peak(peak):
        peak_ref[...] = jnp.broadcast_to(jnp.max(peak, axis=1, keepdims=True), (tall, LANES))

    def begin(owner):
        queries = spread(owner)
        peak = None
        for at in chunks:
            part = score(owner, queries, at)
            peak = part if peak is None else jnp.maximum(peak, part)
        set_peak(peak)

    def finish(owner, after):
        queries = None if after is None else spread(after)
        block_peak = peak_ref[...]
        column = block_peak[:, :1]
        sums = jnp.zeros((tall, chunk_cols), f32)
        values = jnp.zeros((tall, pairs * LANES), f32)
        peak = None
        for at in chunks:
            sums, values = weigh(owner, column, sums, values, at)
            if after is not None:
                part = score(after, queries, at)
                peak = part if peak is None else jnp.maximum(peak, part)
        if after is not None:
            set_peak(peak)
        block_sum = jnp.sum(sums, axis=1, keepdims=True)
        value_ref[...] = jnp.concatenate(
            [
                values[
                    pair * 2 * heads : (pair + 1) * 2 * heads, pair * LANES : (pair + 1) * LANES
                ]
                for pair in range(pairs)
            ],
            axis=0,
        )
        last = jnp.concatenate([last_ref[owner * mine + i] for i in range(mine)], axis=0)
        stat_ref[...] = jnp.where(
            stat_kind == 0, block_peak, jnp.where(stat_kind == 1, block_sum, last)
        )
        stats = jnp.zeros((mine, LANES), f32)
        held = None
        for head in range(heads):
            inside = pl.ds(head, mine, stride=heads)
            stats = jnp.where(part_lane % heads == head, stat_ref[inside, :], stats)
            straight = value_ref[inside, :]
            turned = pltpu.roll(straight, head_size, 1)
            if head % 2 == 0:
                held = jnp.where(even_row, turned, straight)
            else:
                at = (head // 2) * LANES
                part_ref[me, owner, :, at : at + LANES] = jnp.where(
                    low_half, held, jnp.where(even_row, straight, turned)
                ).astype(bf16)
        coarse = stats.astype(bf16).astype(f32)
        medium = (stats - coarse).astype(bf16).astype(f32)
        fine = stats - coarse - medium
        part_ref[me, owner, :, q_cols:] = jnp.where(
            part_lane < segment, coarse, jnp.where(part_lane < 2 * segment, medium, fine)
        ).astype(bf16)
        for step in reversed(range(1, n_kv)):
            part_copy(me, owner, flip(me, step, n_kv)).start()

    begin(me)
    finish(me, None)
    first = flip(me, 1, n_kv)
    ag1_copy(first, me).wait_recv()
    begin(first)

    def attend(step, carry):
        owner, after = flip(me, step, n_kv), flip(me, step + 1, n_kv)
        ag1_copy(after, me).wait_recv()
        finish(owner, after)
        return carry

    lax.fori_loop(1, n_kv - 1, attend, 0)
    finish(flip(me, n_kv - 1, n_kv), None)

    def slot(place):
        return slice(place * mine, (place + 1) * mine)

    for place in range(n_kv):
        other = flip(me, place, n_kv)
        if place > 0:
            new_copy(other, me).wait_recv()
        fresh_ref[slot(place), :] = new_ref[other]
    loads[5].wait()
    for step in range(n_kv):
        for place in range(n_kv):
            source = flip(me, place, n_kv)
            block = flip(me, place ^ step, n_kv)
            if place > 0:
                part_copy(source, block, me).wait_recv()
            gathered_ref[place, slot(place ^ step), :] = part_ref[source, block].astype(f32)

    row_lane = lane_of((rows, LANES))
    fresh = fresh_ref[:, k_pad:]
    stats = []
    for place in range(n_kv):
        stat = gathered_ref[place, :, q_cols:]
        stat = stat + pltpu.roll(stat, LANES - segment, 1) + pltpu.roll(stat, LANES - 2 * segment, 1)
        stats.append(stat)
    last = stats[0]
    for stat in stats[1:]:
        last = last + stat
    cum_query = pltpu.roll(last, LANES - 2 * heads, 1) + pltpu.roll(fresh, LANES - heads, 1)
    new_biased = fresh - cum_query
    peak = new_biased
    for stat in stats:
        peak = jnp.maximum(peak, stat)
    new_weight = jnp.exp(new_biased - peak)
    weight_sum = new_weight
    factors = []
    for stat in stats:
        factor = jnp.exp(stat - peak)
        weight_sum = weight_sum + factor * pltpu.roll(stat, LANES - heads, 1)
        factors.append(factor)
    factors.append(new_weight.astype(bf16).astype(f32))
    log_weight = peak + jnp.log(weight_sum) + cum_query
    scales = []
    for factor in factors:
        scale = factor / weight_sum
        coarse = scale.astype(bf16).astype(f32)
        fine = pltpu.roll(scale - coarse, heads, 1)
        scales.append(
            jnp.where(
                row_lane < heads, coarse, jnp.where(row_lane < 2 * heads, fine, 0.0)
            ).astype(bf16)
        )
    attended = jnp.zeros((rows, q_cols), f32)
    for place, scale in enumerate(scales):
        wide = jnp.dot(scale, head_map, preferred_element_type=f32)
        if place < n_kv:
            attended = attended + wide * gathered_ref[place, :, :q_cols]
        else:
            attended = attended + wide * grouped(fresh_ref[:, :k_pad], q_cols)
    for place in range(n_kv):
        order_ref[flip(me, place, n_kv), :, :q_cols] = attended[slot(place)]
        order_ref[flip(me, place, n_kv), :, q_cols:] = log_weight[slot(place)]
    for owner in range(n_kv):
        fresh_ref[slot(owner), :] = jnp.concatenate(
            [order_ref[owner, :, q_cols:]] * (k_pad // LANES + 1), axis=1
        )
        wide_rows_ref[slot(owner), :] = order_ref[owner, :, :q_cols]
    tp_ref[my_tp] = jnp.dot(
        wide_rows_ref[...].astype(bf16), w_out_ref[...], preferred_element_type=f32
    ).astype(bf16)

    def tp_copy(source, target):
        return pltpu.make_async_remote_copy(
            src_ref=tp_ref.at[source],
            dst_ref=tp_ref.at[source],
            send_sem=tp_send.at[target],
            recv_sem=tp_recv.at[source],
            device_id={"tp": target},
            device_id_type=MESH,
        )

    for step in reversed(range(1, n_tp)):
        tp_copy(my_tp, flip(my_tp, step, n_tp)).start()

    log_ref[...] = fresh_ref[:, :heads]

    def settle(step, carry):
        other = flip(me, step, n_kv)
        rs1_copy(me, other).wait_send()
        ag1_copy(me, other).wait_send()
        new_copy(me, other).wait_send()
        for block in range(n_kv):
            part_copy(me, block, other).wait_send()
        return carry

    lax.fori_loop(1, n_kv, settle, 0)
    for step in range(1, n_tp):
        tp_copy(flip(my_tp, step, n_tp), my_tp).wait_recv()
    mixed = tp_ref[0].astype(f32)
    for source in range(1, n_tp):
        mixed = mixed + tp_ref[source].astype(f32)
    mixed_ref[...] = mixed.astype(bf16)
    for step in range(1, n_tp):
        tp_copy(my_tp, flip(my_tp, step, n_tp)).wait_send()


def shards(
    tokens,
    norm_gain,
    w_query,
    w_key,
    w_value,
    forget_weight,
    forget_bias,
    kv_cache,
    cum_gates,
    lengths,
    w_out,
):
    n_kv, n_tp = lax.axis_size("kv"), lax.axis_size("tp")
    rows, cols = tokens.shape
    span, kv_local, entry = kv_cache.shape[1:]
    heads = cum_gates.shape[1]
    q_cols, k_cols = w_query.shape[1], w_key.shape[1]
    k_pad = -(-k_cols // LANES) * LANES
    wide = q_cols + 2 * k_pad + LANES
    mine = rows // n_kv
    out_cols = w_out.shape[1]
    f32, bf16 = jnp.float32, jnp.bfloat16
    vmem = pl.BlockSpec(memory_space=pltpu.VMEM)
    smem = pl.BlockSpec(memory_space=pltpu.SMEM)
    hbm = pl.BlockSpec(memory_space=pl.ANY)
    dma = pltpu.SemaphoreType.DMA
    tall = (mine * heads, LANES)
    return pl.pallas_call(
        functools.partial(kernel, n_kv, n_tp),
        out_shape=(
            pltpu.VMEM((rows, out_cols), bf16),
            pltpu.VMEM((rows, heads), f32),
        ),
        in_specs=[vmem, vmem, vmem, smem] + [hbm] * 7,
        out_specs=(vmem, vmem),
        scratch_shapes=[
            pltpu.VMEM(w_query.shape, bf16),
            pltpu.VMEM(w_key.shape, bf16),
            pltpu.VMEM(w_value.shape, bf16),
            pltpu.VMEM((LANES, cols), bf16),
            pltpu.VMEM((rows, span * kv_local, entry), bf16),
            pltpu.VMEM(cum_gates.shape, f32),
            pltpu.VMEM(w_out.shape, bf16),
            pltpu.VMEM((rows, heads, span * kv_local), f32),
            pltpu.VMEM((rows, heads, LANES), f32),
            pltpu.VMEM((n_kv, mine, wide), bf16),
            pltpu.VMEM((n_kv, mine, wide), bf16),
            pltpu.VMEM((n_kv, mine, q_cols), bf16),
            pltpu.VMEM((n_kv, mine, k_pad + LANES), f32),
            pltpu.VMEM((1, LANES), f32),
            pltpu.VMEM(tall, f32),
            pltpu.VMEM((mine * heads, span * kv_local), f32),
            pltpu.VMEM(tall, f32),
            pltpu.VMEM(tall, f32),
            pltpu.VMEM(tall, f32),
            pltpu.VMEM((n_kv, n_kv, mine, q_cols + LANES), bf16),
            pltpu.VMEM((n_kv, rows, q_cols + LANES), f32),
            pltpu.VMEM((rows, k_pad + LANES), f32),
            pltpu.VMEM((n_kv, mine, q_cols + LANES), f32),
            pltpu.VMEM((rows, q_cols), f32),
            pltpu.VMEM((n_tp, rows, out_cols), bf16),
            dma((6,)),
            dma((n_kv,)),
        ]
        + [dma((n_kv,))] * 6
        + [dma((n_kv, n_kv))] * 2
        + [dma((n_tp,))] * 2,
        compiler_params=pltpu.CompilerParams(
            collective_id=0, has_side_effects=True, vmem_limit_bytes=56 * 1024 * 1024
        ),
    )(
        tokens,
        norm_gain.reshape(1, cols),
        forget_bias.reshape(1, heads),
        lengths,
        w_query,
        w_key,
        w_value,
        forget_weight.T,
        kv_cache.reshape(rows, span * kv_local, entry),
        cum_gates,
        w_out,
    )


def solution(mesh):
    placed = (
        P(None, "kv"),
        P("kv"),
        P("kv", "tp"),
        P("kv", "tp"),
        P("kv", "tp"),
        P(),
        P("tp"),
        P(None, "kv", "tp", None),
        P(None, "tp", "kv"),
        P(),
        P("tp", "kv"),
    )
    return jax.shard_map(
        shards,
        mesh=mesh,
        in_specs=placed,
        out_specs=(P(None, "kv"), P(None, "tp")),
        check_vma=False,
    )
```

```python
import functools
import jax
import jax.numpy as jnp
from jax import lax
from jax.experimental import pallas as pl
from jax.experimental.pallas import tpu as pltpu
from jax.sharding import PartitionSpec as P

norm_eps = 1e-05
masked_floor = -1e30
LANES = 128
MESH = pl.DeviceIdType.MESH


def flip(index, step, count):
    out = index
    bit = 1
    while bit < count:
        out = out + bit * ((step // bit) % 2) * (1 - 2 * ((index // bit) % 2))
        bit *= 2
    return out


def lane_of(shape):
    return lax.broadcasted_iota(jnp.int32, shape, len(shape) - 1)


def kernel(
    n_kv,
    n_tp,
    tokens_hbm,
    gain_hbm,
    bias_hbm,
    lengths_hbm,
    w_query_hbm,
    w_key_hbm,
    w_value_hbm,
    gate_hbm,
    cache_hbm,
    cum_hbm,
    w_out_hbm,
    mixed_ref,
    log_ref,
    tokens_ref,
    gain_ref,
    bias_ref,
    lengths_ref,
    w_query_ref,
    w_key_ref,
    w_value_ref,
    gate_ref,
    cache_ref,
    cum_ref,
    w_out_ref,
    shift_ref,
    last_ref,
    proj_ref,
    rs1_ref,
    query_ref,
    new_ref,
    bias_pad_ref,
    wide_ref,
    score_ref,
    peak_ref,
    value_ref,
    stat_ref,
    part_ref,
    gathered_ref,
    fresh_ref,
    order_ref,
    wide_rows_ref,
    tp_ref,
    weight_sems,
    cache_sems,
    rs1_send,
    rs1_recv,
    ag1_send,
    ag1_recv,
    new_send,
    new_recv,
    part_send,
    part_recv,
    tp_send,
    tp_recv,
):
    f32, bf16 = jnp.float32, jnp.bfloat16
    me = lax.axis_index("kv")
    my_tp = lax.axis_index("tp")
    rows, cols = tokens_ref.shape
    heads = cum_ref.shape[1]
    span = cum_ref.shape[2]
    entries = cache_ref.shape[1]
    kv_local = entries // span
    group = heads // kv_local
    head_size = LANES // 2
    all_heads = gate_hbm.shape[0]
    mine = rows // n_kv
    pairs = mine // 2
    q_cols = w_query_ref.shape[1]
    k_cols = w_key_ref.shape[1]
    k_pad = -(-k_cols // LANES) * LANES
    model_width = cols * n_kv
    inv_root = head_size ** (-0.5)
    chunk_cols = 2 * LANES
    chunks = range(0, entries, chunk_cols)
    segment = LANES // 4

    offset = pl.multiple_of(me * cols, cols)
    loads = [
        pltpu.make_async_copy(src, dst, weight_sems.at[i])
        for i, (src, dst) in enumerate(
            [
                (tokens_hbm, tokens_ref),
                (gain_hbm, gain_ref),
                (w_query_hbm, w_query_ref),
                (w_key_hbm, w_key_ref),
                (w_value_hbm, w_value_ref),
                (gate_hbm.at[:, pl.ds(offset, cols)], gate_ref.at[pl.ds(0, all_heads)]),
                (bias_hbm, bias_ref),
                (lengths_hbm, lengths_ref),
                (cum_hbm, cum_ref),
                (w_out_hbm, w_out_ref),
            ]
        )
    ]
    barrier = pltpu.get_barrier_semaphore()
    for step in range(1, n_kv):
        pl.semaphore_signal(
            barrier, inc=1, device_id={"kv": flip(me, step, n_kv)}, device_id_type=MESH
        )
    for step in range(1, n_tp):
        pl.semaphore_signal(
            barrier, inc=1, device_id={"tp": flip(my_tp, step, n_tp)}, device_id_type=MESH
        )
    for load in loads[:9]:
        load.start()

    def cache_load(owner):
        at = pl.ds(owner * mine, mine)
        return pltpu.make_async_copy(cache_hbm.at[at], cache_ref.at[at], cache_sems.at[owner])

    gate_ref[all_heads:, :] = jnp.zeros((LANES - all_heads, cols), bf16)
    bias_pad_ref[...] = jnp.zeros_like(bias_pad_ref)
    for load in loads[:2]:
        load.wait()
    tokens_f = tokens_ref[...].astype(f32)
    squares = jnp.sum(tokens_f * tokens_f, axis=1, keepdims=True)
    normed = (tokens_f * gain_ref[...]).astype(bf16)
    for load in loads[2:8]:
        load.wait()
    for step in range(n_kv):
        cache_load(flip(me, step, n_kv)).start()
    loads[9].start()
    bias_pad_ref[:, 0:heads] = bias_ref[...]
    pieces = [jnp.dot(normed, w_query_ref[...], preferred_element_type=f32)]
    for w_ref in (w_key_ref, w_value_ref):
        piece = jnp.dot(normed, w_ref[...], preferred_element_type=f32)
        if k_pad > k_cols:
            piece = jnp.concatenate([piece, jnp.zeros((rows, k_pad - k_cols), f32)], axis=1)
        pieces.append(piece)
    gates = lax.dot_general(
        normed, gate_ref[...], (((1,), (1,)), ((), ())), preferred_element_type=f32
    )
    pieces.append(jnp.where(lane_of(gates.shape) == all_heads, squares, gates))
    at = 0
    for piece in pieces:
        for owner in range(n_kv):
            proj_ref[owner, :, at : at + piece.shape[1]] = piece[
                owner * mine : (owner + 1) * mine
            ].astype(bf16)
        at += piece.shape[1]

    everyone = pl.ds(0, n_kv - 1)

    def rs1_copy(source, target):
        return pltpu.make_async_remote_copy(
            src_ref=proj_ref.at[target],
            dst_ref=rs1_ref.at[source],
            send_sem=rs1_send.at[0],
            recv_sem=rs1_recv.at[0],
            device_id={"kv": target},
            device_id_type=MESH,
        )

    def rs1_all():
        return pltpu.make_async_remote_copy(
            src_ref=proj_ref.at[everyone],
            dst_ref=rs1_ref.at[everyone],
            send_sem=rs1_send.at[0],
            recv_sem=rs1_recv.at[0],
            device_id={"kv": flip(me, 1, n_kv)},
            device_id_type=MESH,
        )

    pl.semaphore_wait(barrier, n_kv + n_tp - 2)
    for step in reversed(range(1, n_kv)):
        rs1_copy(me, flip(me, step, n_kv)).start()

    loads[8].wait()
    tile = (heads, LANES)
    lane = lane_of(tile)
    own_column = (lane % kv_local) == (lax.broadcasted_iota(jnp.int32, tile, 0) // group)

    def prepare(row, carry):
        length = lengths_ref[row] - me * span
        last = jnp.zeros(tile, f32)
        for chunk in range(span // LANES):
            cum = cum_ref[row, :, chunk * LANES : (chunk + 1) * LANES]
            place = lane + chunk * LANES
            shift = jnp.where(place < length, -cum, masked_floor)
            last = last + jnp.where(place == length - 1, cum, 0.0)
            for part in range(kv_local):
                if kv_local == 1:
                    spread = shift
                else:
                    pick = lane // kv_local + part * (LANES // kv_local)
                    spread = jnp.take_along_axis(shift, pick, axis=1)
                    spread = jnp.where(own_column, spread, masked_floor)
                at = (chunk * kv_local + part) * LANES
                shift_ref[row, :, at : at + LANES] = spread
        last_ref[row] = jnp.broadcast_to(jnp.sum(last, axis=1, keepdims=True), tile)
        return carry

    lax.fori_loop(0, rows, prepare, 0, unroll=4)

    total = proj_ref[me].astype(f32)
    rs1_all().wait_recv()
    for step in range(1, n_kv):
        total = total + rs1_ref[flip(me, step, n_kv)].astype(f32)
    misc = total[:, q_cols + 2 * k_pad :]
    part_lane = lane_of((mine, LANES))
    total_sq = jnp.sum(jnp.where(part_lane == all_heads, misc, 0.0), axis=1, keepdims=True)
    row_scale = lax.rsqrt(total_sq / model_width + norm_eps)
    query_ref[me] = (row_scale * total[:, :q_cols]).astype(bf16)

    def ag1_copy(source, target):
        return pltpu.make_async_remote_copy(
            src_ref=query_ref.at[source],
            dst_ref=query_ref.at[source],
            send_sem=ag1_send.at[0],
            recv_sem=ag1_recv.at[source],
            device_id={"kv": target},
            device_id_type=MESH,
        )

    for step in reversed(range(1, n_kv)):
        ag1_copy(me, flip(me, step, n_kv)).start()

    low_half = part_lane < head_size
    even_row = lax.broadcasted_iota(jnp.int32, (mine, LANES), 0) % 2 == 0

    def grouped(values, width):
        tiles = []
        for at in range(0, width, LANES):
            halves = []
            for half in range(2):
                source = (at // head_size + half) // group
                found = values[:, (source // 2) * LANES : (source // 2 + 1) * LANES]
                if source % 2 != half:
                    found = pltpu.roll(found, head_size, 1)
                halves.append(found)
            low = lane_of(halves[0].shape) < head_size
            tiles.append(jnp.where(low, halves[0], halves[1]))
        return jnp.concatenate(tiles, axis=1)

    head_shape = (LANES, q_cols)
    head_map = (
        lax.broadcasted_iota(jnp.int32, head_shape, 0) % heads
        == lax.broadcasted_iota(jnp.int32, head_shape, 1) // head_size
    ).astype(f32).astype(bf16)

    new_key = (row_scale * total[:, q_cols : q_cols + k_pad]).astype(bf16).astype(f32)
    new_value = (row_scale * total[:, q_cols + k_pad : q_cols + 2 * k_pad]).astype(bf16)
    product = query_ref[me].astype(f32) * grouped(new_key, q_cols)
    coarse = product.astype(bf16)
    fine = (product - coarse.astype(f32)).astype(bf16)
    new_score = sum(
        lax.dot_general(part, head_map, (((1,), (1,)), ((), ())), preferred_element_type=f32)
        for part in (coarse, fine)
    )
    gate = pltpu.roll(row_scale * misc, (LANES - my_tp * heads) % LANES, 1) + bias_pad_ref[...]
    log_gate = jnp.minimum(gate, 0.0) - jnp.log1p(jnp.exp(-jnp.abs(gate)))
    new_ref[me, :, :k_pad] = new_value.astype(f32)
    new_ref[me, :, k_pad:] = jnp.where(
        part_lane < heads, new_score * inv_root, pltpu.roll(log_gate, heads, 1)
    )

    def new_copy(source, target):
        return pltpu.make_async_remote_copy(
            src_ref=new_ref.at[source],
            dst_ref=new_ref.at[source],
            send_sem=new_send.at[0],
            recv_sem=new_recv.at[0],
            device_id={"kv": target},
            device_id_type=MESH,
        )

    def new_all():
        return pltpu.make_async_remote_copy(
            src_ref=new_ref.at[everyone],
            dst_ref=new_ref.at[everyone],
            send_sem=new_send.at[0],
            recv_sem=new_recv.at[0],
            device_id={"kv": flip(me, 1, n_kv)},
            device_id_type=MESH,
        )

    for step in reversed(range(1, n_kv)):
        new_copy(me, flip(me, step, n_kv)).start()

    early = n_kv - 2

    def part_copy(source, block, target, stage):
        return pltpu.make_async_remote_copy(
            src_ref=part_ref.at[source, block],
            dst_ref=part_ref.at[source, block],
            send_sem=part_send.at[0],
            recv_sem=part_recv.at[stage],
            device_id={"kv": target},
            device_id_type=MESH,
        )

    def part_all(count, stage):
        some = part_ref.at[pl.ds(0, count), everyone]
        return pltpu.make_async_remote_copy(
            src_ref=some,
            dst_ref=some,
            send_sem=part_send.at[0],
            recv_sem=part_recv.at[stage],
            device_id={"kv": flip(me, 1, n_kv)},
            device_id_type=MESH,
        )

    zeros = jnp.zeros((heads, LANES), f32)
    stat_kind = (lane % segment) // heads

    def cached(row_a, row_b, at):
        inside = slice(at, at + chunk_cols)
        return jnp.concatenate([cache_ref[row_a, inside, :], cache_ref[row_b, inside, :]], axis=1)

    def weigh(pair):
        peak = peak_ref[pair, :, :1]
        sums = jnp.zeros((2 * heads, chunk_cols), f32)
        weights = []
        for at in chunks:
            weight = jnp.exp(score_ref[pair, :, at : at + chunk_cols] - peak)
            sums = sums + weight
            weights.append(weight.astype(bf16))
        return weights, jnp.sum(sums, axis=1, keepdims=True), peak

    def score(owner, pair):
        first, second = 2 * pair, 2 * pair + 1
        row_a, row_b = owner * mine + first, owner * mine + second
        left = wide_ref[first * heads : (first + 1) * heads, :]
        right = wide_ref[second * heads : (second + 1) * heads, :]
        queries = jnp.concatenate(
            [
                jnp.concatenate([left, zeros], axis=1),
                jnp.concatenate([zeros, right], axis=1),
            ],
            axis=0,
        ).astype(bf16)
        peak = None
        for at in chunks:
            part = lax.dot_general(
                queries,
                cached(row_a, row_b, at),
                (((1,), (1,)), ((), ())),
                preferred_element_type=f32,
            )
            part = part + jnp.concatenate(
                [shift_ref[row_a, :, at : at + chunk_cols], shift_ref[row_b, :, at : at + chunk_cols]],
                axis=0,
            )
            score_ref[pair, :, at : at + chunk_cols] = part
            peak = part if peak is None else jnp.maximum(peak, part)
        peak_ref[pair] = jnp.broadcast_to(
            jnp.max(peak, axis=1, keepdims=True), (2 * heads, LANES)
        )

    def gather(owner, pair, weights, total_weight, peak):
        first, second = 2 * pair, 2 * pair + 1
        row_a, row_b = owner * mine + first, owner * mine + second
        values = jnp.zeros((2 * heads, chunk_cols), f32)
        for weight, at in zip(weights, chunks):
            values = values + jnp.dot(
                weight, cached(row_a, row_b, at), preferred_element_type=f32
            )
        for i, (place, row) in enumerate(((first, row_a), (second, row_b))):
            inside = slice(i * heads, (i + 1) * heads)
            place_rows = slice(place * heads, (place + 1) * heads)
            value_ref[place_rows, :] = values[inside, i * LANES : (i + 1) * LANES]
            stat_ref[place_rows, :] = jnp.where(
                stat_kind == 0,
                peak[inside],
                jnp.where(stat_kind == 1, total_weight[inside], last_ref[row]),
            )

    def ready(owner):
        cache_load(owner).wait()
        query = query_ref[owner].astype(f32) * inv_root
        for head in range(heads):
            at = (head // 2) * LANES
            found = query[:, at : at + LANES]
            if head % 2 == 1:
                found = pltpu.roll(found, head_size, 1)
            wide_ref[pl.ds(head, mine, stride=heads), :] = jnp.where(low_half, found, 0.0)

    def send(owner, stage):
        stats = jnp.zeros((mine, LANES), f32)
        held = None
        for head in range(heads):
            inside = pl.ds(head, mine, stride=heads)
            stats = jnp.where(part_lane % heads == head, stat_ref[inside, :], stats)
            found = value_ref[inside, :]
            if head % 2 == 0:
                held = pltpu.roll(found, head_size, 1)
            else:
                at = (head // 2) * LANES
                part_ref[me, owner, :, at : at + LANES] = jnp.where(low_half, held, found).astype(
                    bf16
                )
        coarse = stats.astype(bf16).astype(f32)
        medium = (stats - coarse).astype(bf16).astype(f32)
        fine = stats - coarse - medium
        part_ref[me, owner, :, q_cols:] = jnp.where(
            part_lane < segment, coarse, jnp.where(part_lane < 2 * segment, medium, fine)
        ).astype(bf16)
        for step in reversed(range(1, n_kv)):
            part_copy(me, owner, flip(me, step, n_kv), stage).start()

    ready(me)
    for pair in range(pairs):
        score(me, pair)
    for pair in range(pairs):
        gather(me, pair, *weigh(pair))
    send(me, 0)
    first = flip(me, 1, n_kv)
    ag1_copy(first, me).wait_recv()
    ready(first)
    for pair in range(pairs):
        score(first, pair)

    def attend(step, carry):
        owner, after = flip(me, step, n_kv), flip(me, step + 1, n_kv)
        ag1_copy(after, me).wait_recv()
        ready(after)
        for pair in range(pairs):
            weights = weigh(pair)
            score(after, pair)
            gather(owner, pair, *weights)
        send(owner, step // early)
        return carry

    lax.fori_loop(1, n_kv - 1, attend, 0)
    final = flip(me, n_kv - 1, n_kv)
    for pair in range(pairs):
        gather(final, pair, *weigh(pair))
    send(final, 1)

    def slot(place):
        return slice(place * mine, (place + 1) * mine)

    new_all().wait_recv()
    for place in range(n_kv):
        fresh_ref[slot(place), :] = new_ref[flip(me, place, n_kv)]
    loads[9].wait()
    for step in range(n_kv):
        if step == 0:
            part_all(early, 0).wait_recv()
        if step == early:
            part_all(n_kv - early, 1).wait_recv()
        for place in range(n_kv):
            source = flip(me, place, n_kv)
            block = flip(me, place ^ step, n_kv)
            gathered_ref[place, slot(place ^ step), :] = part_ref[source, block].astype(f32)

    row_lane = lane_of((rows, LANES))
    fresh = fresh_ref[:, k_pad:]
    stats = []
    for place in range(n_kv):
        stat = gathered_ref[place, :, q_cols:]
        stat = stat + pltpu.roll(stat, LANES - segment, 1) + pltpu.roll(stat, LANES - 2 * segment, 1)
        stats.append(stat)
    last = stats[0]
    for stat in stats[1:]:
        last = last + stat
    cum_query = pltpu.roll(last, LANES - 2 * heads, 1) + pltpu.roll(fresh, LANES - heads, 1)
    new_biased = fresh - cum_query
    peak = new_biased
    for stat in stats:
        peak = jnp.maximum(peak, stat)
    new_weight = jnp.exp(new_biased - peak)
    weight_sum = new_weight
    factors = []
    for stat in stats:
        factor = jnp.exp(stat - peak)
        weight_sum = weight_sum + factor * pltpu.roll(stat, LANES - heads, 1)
        factors.append(factor)
    factors.append(new_weight.astype(bf16).astype(f32))
    inverse = 1.0 / weight_sum
    scales = []
    for factor in factors:
        scale = factor * inverse
        coarse = scale.astype(bf16).astype(f32)
        fine = pltpu.roll(scale - coarse, heads, 1)
        scales.append(
            jnp.where(
                row_lane < heads, coarse, jnp.where(row_lane < 2 * heads, fine, 0.0)
            ).astype(bf16)
        )
    attended = jnp.zeros((rows, q_cols), f32)
    for place, scale in enumerate(scales):
        wide = jnp.dot(scale, head_map, preferred_element_type=f32)
        if place < n_kv:
            attended = attended + wide * gathered_ref[place, :, :q_cols]
        else:
            attended = attended + wide * grouped(fresh_ref[:, :k_pad], q_cols)
    for place in range(n_kv):
        order_ref[flip(me, place, n_kv), :, :q_cols] = attended[slot(place)]
    for owner in range(n_kv):
        wide_rows_ref[slot(owner), :] = order_ref[owner, :, :q_cols]
    tp_ref[my_tp] = jnp.dot(
        wide_rows_ref[...].astype(bf16), w_out_ref[...], preferred_element_type=f32
    ).astype(bf16)

    def tp_copy(source, target):
        return pltpu.make_async_remote_copy(
            src_ref=tp_ref.at[source],
            dst_ref=tp_ref.at[source],
            send_sem=tp_send.at[0],
            recv_sem=tp_recv.at[0],
            device_id={"tp": target},
            device_id_type=MESH,
        )

    def tp_all():
        some = tp_ref.at[pl.ds(0, n_tp - 1)]
        return pltpu.make_async_remote_copy(
            src_ref=some,
            dst_ref=some,
            send_sem=tp_send.at[0],
            recv_sem=tp_recv.at[0],
            device_id={"tp": flip(my_tp, 1, n_tp)},
            device_id_type=MESH,
        )

    for step in reversed(range(1, n_tp)):
        tp_copy(my_tp, flip(my_tp, step, n_tp)).start()

    log_weight = peak + jnp.log(weight_sum) + cum_query
    for place in range(n_kv):
        order_ref[flip(me, place, n_kv), :, q_cols:] = log_weight[slot(place)]
    for owner in range(n_kv):
        fresh_ref[slot(owner), k_pad:] = order_ref[owner, :, q_cols:]
    log_ref[...] = jnp.transpose(fresh_ref[:, k_pad:])[:heads]

    rs1_all().wait_send()
    pltpu.make_async_remote_copy(
        src_ref=query_ref.at[everyone],
        dst_ref=query_ref.at[everyone],
        send_sem=ag1_send.at[0],
        recv_sem=ag1_recv.at[0],
        device_id={"kv": flip(me, 1, n_kv)},
        device_id_type=MESH,
    ).wait_send()
    new_all().wait_send()
    part_all(n_kv, 0).wait_send()
    tp_all().wait_recv()
    mixed = tp_ref[0].astype(f32)
    for source in range(1, n_tp):
        mixed = mixed + tp_ref[source].astype(f32)
    mixed_ref[...] = mixed.astype(bf16)
    tp_all().wait_send()


def shards(
    tokens,
    norm_gain,
    w_query,
    w_key,
    w_value,
    forget_weight,
    forget_bias,
    kv_cache,
    cum_gates,
    lengths,
    w_out,
):
    n_kv, n_tp = lax.axis_size("kv"), lax.axis_size("tp")
    rows, cols = tokens.shape
    span, kv_local, entry = kv_cache.shape[1:]
    heads = cum_gates.shape[1]
    q_cols, k_cols = w_query.shape[1], w_key.shape[1]
    k_pad = -(-k_cols // LANES) * LANES
    wide = q_cols + 2 * k_pad + LANES
    mine = rows // n_kv
    out_cols = w_out.shape[1]
    f32, bf16 = jnp.float32, jnp.bfloat16
    vmem = pl.BlockSpec(memory_space=pltpu.VMEM)
    hbm = pl.BlockSpec(memory_space=pl.ANY)
    dma = pltpu.SemaphoreType.DMA
    tall = (mine * heads, LANES)
    mixed, log_weight = pl.pallas_call(
        functools.partial(kernel, n_kv, n_tp),
        out_shape=(
            pltpu.VMEM((rows, out_cols), bf16),
            pltpu.VMEM((heads, rows), f32),
        ),
        in_specs=[hbm] * 11,
        out_specs=(vmem, vmem),
        scratch_shapes=[
            pltpu.VMEM(tokens.shape, bf16),
            pltpu.VMEM((1, cols), f32),
            pltpu.VMEM((1, heads), f32),
            pltpu.SMEM(lengths.shape, jnp.int32),
            pltpu.VMEM(w_query.shape, bf16),
            pltpu.VMEM(w_key.shape, bf16),
            pltpu.VMEM(w_value.shape, bf16),
            pltpu.VMEM((LANES, cols), bf16),
            pltpu.VMEM((rows, span * kv_local, entry), bf16),
            pltpu.VMEM(cum_gates.shape, f32),
            pltpu.VMEM(w_out.shape, bf16),
            pltpu.VMEM((rows, heads, span * kv_local), f32),
            pltpu.VMEM((rows, heads, LANES), f32),
            pltpu.VMEM((n_kv, mine, wide), bf16),
            pltpu.VMEM((n_kv, mine, wide), bf16),
            pltpu.VMEM((n_kv, mine, q_cols), bf16),
            pltpu.VMEM((n_kv, mine, k_pad + LANES), f32),
            pltpu.VMEM((1, LANES), f32),
            pltpu.VMEM(tall, f32),
            pltpu.VMEM((mine // 2, 2 * heads, span * kv_local), f32),
            pltpu.VMEM((mine // 2, 2 * heads, LANES), f32),
            pltpu.VMEM(tall, f32),
            pltpu.VMEM(tall, f32),
            pltpu.VMEM((n_kv, n_kv, mine, q_cols + LANES), bf16),
            pltpu.VMEM((n_kv, rows, q_cols + LANES), f32),
            pltpu.VMEM((rows, k_pad + LANES), f32),
            pltpu.VMEM((n_kv, mine, q_cols + LANES), f32),
            pltpu.VMEM((rows, q_cols), f32),
            pltpu.VMEM((n_tp, rows, out_cols), bf16),
            dma((10,)),
            dma((n_kv,)),
            dma((1,)),
            dma((1,)),
            dma((1,)),
            dma((n_kv,)),
            dma((1,)),
            dma((1,)),
            dma((1,)),
            dma((2,)),
            dma((1,)),
            dma((1,)),
        ],
        compiler_params=pltpu.CompilerParams(
            collective_id=0, has_side_effects=True, vmem_limit_bytes=56 * 1024 * 1024
        ),
    )(
        tokens,
        norm_gain.reshape(1, cols),
        forget_bias.reshape(1, heads),
        lengths,
        w_query,
        w_key,
        w_value,
        forget_weight.T,
        kv_cache.reshape(rows, span * kv_local, entry),
        cum_gates,
        w_out,
    )
    return mixed, log_weight.T


def solution(mesh):
    placed = (
        P(None, "kv"),
        P("kv"),
        P("kv", "tp"),
        P("kv", "tp"),
        P("kv", "tp"),
        P(),
        P("tp"),
        P(None, "kv", "tp", None),
        P(None, "tp", "kv"),
        P(),
        P("tp", "kv"),
    )
    return jax.shard_map(
        shards,
        mesh=mesh,
        in_specs=placed,
        out_specs=(P(None, "kv"), P(None, "tp")),
        check_vma=False,
    )
```

```python
import functools
import jax
import jax.numpy as jnp
from jax import lax
from jax.experimental import pallas as pl
from jax.experimental.pallas import tpu as pltpu
from jax.sharding import PartitionSpec as P

norm_eps = 1e-05
masked_floor = -1e30
LANES = 128
MESH = pl.DeviceIdType.MESH


def flip(index, step, count):
    out = index
    bit = 1
    while bit < count:
        out = out + bit * ((step // bit) % 2) * (1 - 2 * ((index // bit) % 2))
        bit *= 2
    return out


def lane_of(shape):
    return lax.broadcasted_iota(jnp.int32, shape, len(shape) - 1)


def kernel(
    n_kv,
    n_tp,
    tokens_hbm,
    gain_hbm,
    bias_hbm,
    lengths_hbm,
    w_query_hbm,
    w_key_hbm,
    w_value_hbm,
    gate_hbm,
    cache_hbm,
    cum_hbm,
    w_out_hbm,
    mixed_ref,
    log_ref,
    tokens_ref,
    gain_ref,
    bias_ref,
    lengths_ref,
    w_query_ref,
    w_key_ref,
    w_value_ref,
    gate_ref,
    cache_ref,
    cum_ref,
    w_out_ref,
    turned_ref,
    shift_ref,
    last_ref,
    proj_ref,
    rs1_ref,
    query_ref,
    new_ref,
    bias_pad_ref,
    wide_ref,
    score_ref,
    peak_ref,
    value_ref,
    stat_ref,
    part_ref,
    gathered_ref,
    fresh_ref,
    order_ref,
    wide_rows_ref,
    tp_ref,
    weight_sems,
    cache_sems,
    rs1_send,
    rs1_recv,
    ag1_send,
    ag1_recv,
    new_send,
    new_recv,
    part_send,
    part_recv,
    tp_send,
    tp_recv,
):
    f32, bf16 = jnp.float32, jnp.bfloat16
    me = lax.axis_index("kv")
    my_tp = lax.axis_index("tp")
    rows, cols = tokens_ref.shape
    heads = cum_ref.shape[1]
    span = cum_ref.shape[2]
    entries = cache_ref.shape[1]
    kv_local = entries // span
    group = heads // kv_local
    head_size = LANES // 2
    all_heads = gate_hbm.shape[0]
    mine = rows // n_kv
    pairs = mine // 2
    q_cols = w_query_ref.shape[1]
    k_cols = w_key_ref.shape[1]
    k_pad = -(-k_cols // LANES) * LANES
    model_width = cols * n_kv
    inv_root = head_size ** (-0.5)
    chunk_cols = 2 * LANES
    chunks = range(0, entries, chunk_cols)
    segment = LANES // 4

    offset = pl.multiple_of(me * cols, cols)
    loads = [
        pltpu.make_async_copy(src, dst, weight_sems.at[i])
        for i, (src, dst) in enumerate(
            [
                (tokens_hbm, tokens_ref),
                (gain_hbm, gain_ref),
                (w_query_hbm, w_query_ref),
                (w_key_hbm, w_key_ref),
                (w_value_hbm, w_value_ref),
                (gate_hbm.at[:, pl.ds(offset, cols)], gate_ref.at[pl.ds(0, all_heads)]),
                (bias_hbm, bias_ref),
                (lengths_hbm, lengths_ref),
                (cum_hbm, cum_ref),
                (w_out_hbm, w_out_ref),
            ]
        )
    ]
    barrier = pltpu.get_barrier_semaphore()
    for step in range(1, n_kv):
        pl.semaphore_signal(
            barrier, inc=1, device_id={"kv": flip(me, step, n_kv)}, device_id_type=MESH
        )
    for step in range(1, n_tp):
        pl.semaphore_signal(
            barrier, inc=1, device_id={"tp": flip(my_tp, step, n_tp)}, device_id_type=MESH
        )
    for load in loads[:9]:
        load.start()

    def cache_load(owner):
        at = pl.ds(owner * mine, mine)
        return pltpu.make_async_copy(cache_hbm.at[at], cache_ref.at[at], cache_sems.at[owner])

    gate_ref[all_heads:, :] = jnp.zeros((LANES - all_heads, cols), bf16)
    bias_pad_ref[...] = jnp.zeros_like(bias_pad_ref)
    for load in loads[:2]:
        load.wait()
    tokens_f = tokens_ref[...].astype(f32)
    squares = jnp.sum(tokens_f * tokens_f, axis=1, keepdims=True)
    normed = (tokens_f * gain_ref[...]).astype(bf16)
    for load in loads[2:8]:
        load.wait()
    for step in range(n_kv):
        cache_load(flip(me, step, n_kv)).start()
    loads[9].start()
    bias_pad_ref[:, 0:heads] = bias_ref[...]
    pieces = [jnp.dot(normed, w_query_ref[...], preferred_element_type=f32)]
    for w_ref in (w_key_ref, w_value_ref):
        piece = jnp.dot(normed, w_ref[...], preferred_element_type=f32)
        if k_pad > k_cols:
            piece = jnp.concatenate([piece, jnp.zeros((rows, k_pad - k_cols), f32)], axis=1)
        pieces.append(piece)
    gates = lax.dot_general(
        normed, gate_ref[...], (((1,), (1,)), ((), ())), preferred_element_type=f32
    )
    pieces.append(jnp.where(lane_of(gates.shape) == all_heads, squares, gates))
    at = 0
    for piece in pieces:
        for owner in range(n_kv):
            proj_ref[owner, :, at : at + piece.shape[1]] = piece[
                owner * mine : (owner + 1) * mine
            ].astype(bf16)
        at += piece.shape[1]

    everyone = pl.ds(0, n_kv - 1)

    def rs1_copy(source, target):
        return pltpu.make_async_remote_copy(
            src_ref=proj_ref.at[target],
            dst_ref=rs1_ref.at[source],
            send_sem=rs1_send.at[0],
            recv_sem=rs1_recv.at[0],
            device_id={"kv": target},
            device_id_type=MESH,
        )

    def rs1_all():
        return pltpu.make_async_remote_copy(
            src_ref=proj_ref.at[everyone],
            dst_ref=rs1_ref.at[everyone],
            send_sem=rs1_send.at[0],
            recv_sem=rs1_recv.at[0],
            device_id={"kv": flip(me, 1, n_kv)},
            device_id_type=MESH,
        )

    loads[8].wait()
    tile = (heads, LANES)
    lane = lane_of(tile)
    own_column = (lane % kv_local) == (lax.broadcasted_iota(jnp.int32, tile, 0) // group)

    def prepare(row, carry):
        length = lengths_ref[row] - me * span
        last = jnp.zeros(tile, f32)
        for chunk in range(span // LANES):
            cum = cum_ref[row, :, chunk * LANES : (chunk + 1) * LANES]
            place = lane + chunk * LANES
            shift = jnp.where(place < length, -cum, masked_floor)
            last = last + jnp.where(place == length - 1, cum, 0.0)
            for part in range(kv_local):
                if kv_local == 1:
                    spread = shift
                else:
                    pick = lane // kv_local + part * (LANES // kv_local)
                    spread = jnp.take_along_axis(shift, pick, axis=1)
                    spread = jnp.where(own_column, spread, masked_floor)
                at = (chunk * kv_local + part) * LANES
                shift_ref[row, :, at : at + LANES] = spread
        last_ref[row] = jnp.broadcast_to(jnp.sum(last, axis=1, keepdims=True), tile)
        return carry

    def prepare_four(i, carry):
        for j in range(4):
            prepare(4 * i + j, carry)
        return carry

    split = (rows // 8) * ((n_kv + n_kv // 4 - 1 - me) // (n_kv - n_kv // 8))
    split = split + (rows // 8) * ((n_kv + n_kv // 2 - 1 - me) // (n_kv - n_kv // 8))
    lax.fori_loop(0, split, prepare_four, 0)
    pl.semaphore_wait(barrier, n_kv + n_tp - 2)
    for step in reversed(range(1, n_kv)):
        rs1_copy(me, flip(me, step, n_kv)).start()
    lax.fori_loop(split, rows // 4, prepare_four, 0)

    def cached(row_a, row_b, at):
        inside = slice(at, at + chunk_cols)
        return jnp.concatenate([cache_ref[row_a, inside, :], cache_ref[row_b, inside, :]], axis=1)

    pick_shape = (LANES, 2 * LANES)
    pick_row = lax.broadcasted_iota(jnp.int32, pick_shape, 0)
    pick = (
        lane_of(pick_shape) == pick_row + (pick_row // head_size) * head_size
    ).astype(f32).astype(bf16)

    def turn(step, carry):
        owner = flip(me, step, n_kv)
        cache_load(owner).wait()
        for pair in range(pairs):
            row = owner * mine + 2 * pair
            for at in chunks:
                turned_ref[step - 1, pair * LANES : (pair + 1) * LANES, at : at + chunk_cols] = (
                    lax.dot_general(
                        pick,
                        cached(row, row + 1, at),
                        (((1,), (1,)), ((), ())),
                        preferred_element_type=f32,
                    ).astype(bf16)
                )
        return carry

    ahead = turned_ref.shape[0]
    lax.fori_loop(1, ahead + 1, turn, 0)

    total = proj_ref[me].astype(f32)
    rs1_all().wait_recv()
    for step in range(1, n_kv):
        total = total + rs1_ref[flip(me, step, n_kv)].astype(f32)
    misc = total[:, q_cols + 2 * k_pad :]
    part_lane = lane_of((mine, LANES))
    total_sq = jnp.sum(jnp.where(part_lane == all_heads, misc, 0.0), axis=1, keepdims=True)
    row_scale = lax.rsqrt(total_sq / model_width + norm_eps)
    query_ref[me] = (row_scale * total[:, :q_cols]).astype(bf16)

    def ag1_copy(source, target):
        return pltpu.make_async_remote_copy(
            src_ref=query_ref.at[source],
            dst_ref=query_ref.at[source],
            send_sem=ag1_send.at[0],
            recv_sem=ag1_recv.at[source],
            device_id={"kv": target},
            device_id_type=MESH,
        )

    for step in reversed(range(1, n_kv)):
        ag1_copy(me, flip(me, step, n_kv)).start()

    low_half = part_lane < head_size
    even_row = lax.broadcasted_iota(jnp.int32, (mine, LANES), 0) % 2 == 0

    def grouped(values, width):
        tiles = []
        for at in range(0, width, LANES):
            halves = []
            for half in range(2):
                source = (at // head_size + half) // group
                found = values[:, (source // 2) * LANES : (source // 2 + 1) * LANES]
                if source % 2 != half:
                    found = pltpu.roll(found, head_size, 1)
                halves.append(found)
            low = lane_of(halves[0].shape) < head_size
            tiles.append(jnp.where(low, halves[0], halves[1]))
        return jnp.concatenate(tiles, axis=1)

    head_shape = (LANES, q_cols)
    head_map = (
        lax.broadcasted_iota(jnp.int32, head_shape, 0) % heads
        == lax.broadcasted_iota(jnp.int32, head_shape, 1) // head_size
    ).astype(f32).astype(bf16)

    new_key = (row_scale * total[:, q_cols : q_cols + k_pad]).astype(bf16).astype(f32)
    new_value = (row_scale * total[:, q_cols + k_pad : q_cols + 2 * k_pad]).astype(bf16)
    product = query_ref[me].astype(f32) * grouped(new_key, q_cols)
    coarse = product.astype(bf16)
    fine = (product - coarse.astype(f32)).astype(bf16)
    new_score = sum(
        lax.dot_general(part, head_map, (((1,), (1,)), ((), ())), preferred_element_type=f32)
        for part in (coarse, fine)
    )
    gate = pltpu.roll(row_scale * misc, (LANES - my_tp * heads) % LANES, 1) + bias_pad_ref[...]
    log_gate = jnp.minimum(gate, 0.0) - jnp.log1p(jnp.exp(-jnp.abs(gate)))
    new_ref[me, :, :k_pad] = new_value.astype(f32)
    new_ref[me, :, k_pad:] = jnp.where(
        part_lane < heads, new_score * inv_root, pltpu.roll(log_gate, heads, 1)
    )

    def new_copy(source, target):
        return pltpu.make_async_remote_copy(
            src_ref=new_ref.at[source],
            dst_ref=new_ref.at[source],
            send_sem=new_send.at[0],
            recv_sem=new_recv.at[0],
            device_id={"kv": target},
            device_id_type=MESH,
        )

    def new_all():
        return pltpu.make_async_remote_copy(
            src_ref=new_ref.at[everyone],
            dst_ref=new_ref.at[everyone],
            send_sem=new_send.at[0],
            recv_sem=new_recv.at[0],
            device_id={"kv": flip(me, 1, n_kv)},
            device_id_type=MESH,
        )

    for step in reversed(range(1, n_kv)):
        new_copy(me, flip(me, step, n_kv)).start()

    early = n_kv - 2

    def part_copy(source, block, target, stage):
        return pltpu.make_async_remote_copy(
            src_ref=part_ref.at[source, block],
            dst_ref=part_ref.at[source, block],
            send_sem=part_send.at[0],
            recv_sem=part_recv.at[stage],
            device_id={"kv": target},
            device_id_type=MESH,
        )

    def part_all(count, stage):
        some = part_ref.at[pl.ds(0, count), everyone]
        return pltpu.make_async_remote_copy(
            src_ref=some,
            dst_ref=some,
            send_sem=part_send.at[0],
            recv_sem=part_recv.at[stage],
            device_id={"kv": flip(me, 1, n_kv)},
            device_id_type=MESH,
        )

    zeros = jnp.zeros((heads, LANES), f32)
    tall_pair = lax.broadcasted_iota(jnp.int32, (mine * heads, LANES), 0) // (2 * heads)
    stat_kind = (lane % segment) // heads

    def weigh(pair, buffer):
        peak = peak_ref[buffer, pair, :, :1]
        sums = jnp.zeros((2 * heads, chunk_cols), f32)
        weights = []
        for at in chunks:
            weight = jnp.exp(score_ref[buffer, pair, :, at : at + chunk_cols] - peak)
            sums = sums + weight
            weights.append(weight.astype(bf16))
        return weights, jnp.sum(sums, axis=1, keepdims=True), peak

    def shifts(row, count, at):
        return jnp.concatenate(
            [shift_ref[row + i, :, at : at + chunk_cols] for i in range(count)], axis=0
        )

    def score(owner, pair, buffer):
        first, second = 2 * pair, 2 * pair + 1
        row_a, row_b = owner * mine + first, owner * mine + second
        left = wide_ref[first * heads : (first + 1) * heads, :]
        right = wide_ref[second * heads : (second + 1) * heads, :]
        queries = jnp.concatenate(
            [
                jnp.concatenate([left, zeros], axis=1),
                jnp.concatenate([zeros, right], axis=1),
            ],
            axis=0,
        ).astype(bf16)
        peak = None
        for at in chunks:
            part = lax.dot_general(
                queries,
                cached(row_a, row_b, at),
                (((1,), (1,)), ((), ())),
                preferred_element_type=f32,
            )
            part = part + shifts(row_a, 2, at)
            score_ref[buffer, pair, :, at : at + chunk_cols] = part
            peak = part if peak is None else jnp.maximum(peak, part)
        peak_ref[buffer, pair] = jnp.broadcast_to(
            jnp.max(peak, axis=1, keepdims=True), (2 * heads, LANES)
        )

    def score_turned(step, buffer):
        owner = flip(me, step, n_kv)
        query = query_ref[owner].astype(f32) * inv_root
        for head in range(heads):
            at = (head // 2) * LANES
            found = query[:, at : at + LANES]
            other = pltpu.roll(found, head_size, 1)
            low, high = (found, other) if head % 2 == 0 else (other, found)
            wide_ref[pl.ds(head, mine, stride=heads), :] = jnp.where(
                even_row, jnp.where(low_half, low, 0.0), jnp.where(low_half, 0.0, high)
            )
        wide = wide_ref[...]
        queries = jnp.concatenate(
            [jnp.where(tall_pair == pair, wide, 0.0) for pair in range(pairs)], axis=1
        ).astype(bf16)
        peak = None
        for at in chunks:
            part = jnp.dot(
                queries,
                turned_ref[step - 1, :, at : at + chunk_cols],
                preferred_element_type=f32,
            )
            part = part + shifts(owner * mine, mine, at)
            for pair in range(pairs):
                score_ref[buffer, pair, :, at : at + chunk_cols] = part[
                    pair * 2 * heads : (pair + 1) * 2 * heads
                ]
            peak = part if peak is None else jnp.maximum(peak, part)
        peak = jnp.broadcast_to(jnp.max(peak, axis=1, keepdims=True), (mine * heads, LANES))
        for pair in range(pairs):
            peak_ref[buffer, pair] = peak[pair * 2 * heads : (pair + 1) * 2 * heads]

    def gather(owner, pair, weights, total_weight, peak):
        first, second = 2 * pair, 2 * pair + 1
        row_a, row_b = owner * mine + first, owner * mine + second
        values = jnp.zeros((2 * heads, chunk_cols), f32)
        for weight, at in zip(weights, chunks):
            values = values + jnp.dot(
                weight, cached(row_a, row_b, at), preferred_element_type=f32
            )
        for i, (place, row) in enumerate(((first, row_a), (second, row_b))):
            inside = slice(i * heads, (i + 1) * heads)
            place_rows = slice(place * heads, (place + 1) * heads)
            value_ref[place_rows, :] = values[inside, i * LANES : (i + 1) * LANES]
            stat_ref[place_rows, :] = jnp.where(
                stat_kind == 0,
                peak[inside],
                jnp.where(stat_kind == 1, total_weight[inside], last_ref[row]),
            )

    def ready(owner):
        query = query_ref[owner].astype(f32) * inv_root
        for head in range(heads):
            at = (head // 2) * LANES
            found = query[:, at : at + LANES]
            if head % 2 == 1:
                found = pltpu.roll(found, head_size, 1)
            wide_ref[pl.ds(head, mine, stride=heads), :] = jnp.where(low_half, found, 0.0)

    def send(owner, stage):
        stats = jnp.zeros((mine, LANES), f32)
        held = None
        for head in range(heads):
            inside = pl.ds(head, mine, stride=heads)
            stats = jnp.where(part_lane % heads == head, stat_ref[inside, :], stats)
            found = value_ref[inside, :]
            if head % 2 == 0:
                held = pltpu.roll(found, head_size, 1)
            else:
                at = (head // 2) * LANES
                part_ref[me, owner, :, at : at + LANES] = jnp.where(low_half, held, found).astype(
                    bf16
                )
        coarse = stats.astype(bf16).astype(f32)
        medium = (stats - coarse).astype(bf16).astype(f32)
        fine = stats - coarse - medium
        part_ref[me, owner, :, q_cols:] = jnp.where(
            part_lane < segment, coarse, jnp.where(part_lane < 2 * segment, medium, fine)
        ).astype(bf16)
        for step in reversed(range(1, n_kv)):
            part_copy(me, owner, flip(me, step, n_kv), stage).start()

    cache_load(me).wait()
    ready(me)
    for pair in range(pairs):
        score(me, pair, 0)
    for pair in range(pairs):
        gather(me, pair, *weigh(pair, 0))
    send(me, 0)
    ag1_copy(flip(me, 1, n_kv), me).wait_recv()
    score_turned(1, 0)
    for step in range(1, ahead):
        ag1_copy(flip(me, step + 1, n_kv), me).wait_recv()
        owner = flip(me, step, n_kv)
        now, later = (step - 1) % 2, step % 2
        score_turned(step + 1, later)
        for pair in range(pairs):
            gather(owner, pair, *weigh(pair, now))
        send(owner, 0)
    last_buffer = (ahead - 1) % 2

    def attend(step, carry):
        owner, after = flip(me, step, n_kv), flip(me, step + 1, n_kv)
        cache_load(after).wait()
        ag1_copy(after, me).wait_recv()
        ready(after)
        for pair in range(pairs):
            weights = weigh(pair, last_buffer)
            score(after, pair, last_buffer)
            gather(owner, pair, *weights)
        send(owner, step // early)
        return carry

    lax.fori_loop(ahead, n_kv - 1, attend, 0)
    final = flip(me, n_kv - 1, n_kv)
    for pair in range(pairs):
        gather(final, pair, *weigh(pair, last_buffer))
    send(final, 1)

    def slot(place):
        return slice(place * mine, (place + 1) * mine)

    new_all().wait_recv()
    for place in range(n_kv):
        fresh_ref[slot(place), :] = new_ref[flip(me, place, n_kv)]
    loads[9].wait()
    for step in range(n_kv):
        if step == 0:
            part_all(early, 0).wait_recv()
        if step == early:
            part_all(n_kv - early, 1).wait_recv()
        for place in range(n_kv):
            source = flip(me, place, n_kv)
            block = flip(me, place ^ step, n_kv)
            gathered_ref[place, slot(place ^ step), :] = part_ref[source, block].astype(f32)

    row_lane = lane_of((rows, LANES))
    fresh = fresh_ref[:, k_pad:]
    stats = []
    for place in range(n_kv):
        stat = gathered_ref[place, :, q_cols:]
        stat = stat + pltpu.roll(stat, LANES - segment, 1) + pltpu.roll(stat, LANES - 2 * segment, 1)
        stats.append(stat)
    last = stats[0]
    for stat in stats[1:]:
        last = last + stat
    cum_query = pltpu.roll(last, LANES - 2 * heads, 1) + pltpu.roll(fresh, LANES - heads, 1)
    new_biased = fresh - cum_query
    peak = new_biased
    for stat in stats:
        peak = jnp.maximum(peak, stat)
    new_weight = jnp.exp(new_biased - peak)
    weight_sum = new_weight
    factors = []
    for stat in stats:
        factor = jnp.exp(stat - peak)
        weight_sum = weight_sum + factor * pltpu.roll(stat, LANES - heads, 1)
        factors.append(factor)
    factors.append(new_weight.astype(bf16).astype(f32))
    inverse = 1.0 / weight_sum
    scales = []
    for factor in factors:
        scale = factor * inverse
        coarse = scale.astype(bf16).astype(f32)
        fine = pltpu.roll(scale - coarse, heads, 1)
        scales.append(
            jnp.where(
                row_lane < heads, coarse, jnp.where(row_lane < 2 * heads, fine, 0.0)
            ).astype(bf16)
        )
    attended = jnp.zeros((rows, q_cols), f32)
    for place, scale in enumerate(scales):
        wide = jnp.dot(scale, head_map, preferred_element_type=f32)
        if place < n_kv:
            attended = attended + wide * gathered_ref[place, :, :q_cols]
        else:
            attended = attended + wide * grouped(fresh_ref[:, :k_pad], q_cols)
    for place in range(n_kv):
        order_ref[flip(me, place, n_kv), :, :q_cols] = attended[slot(place)]
    for owner in range(n_kv):
        wide_rows_ref[slot(owner), :] = order_ref[owner, :, :q_cols]
    tp_ref[my_tp] = jnp.dot(
        wide_rows_ref[...].astype(bf16), w_out_ref[...], preferred_element_type=f32
    ).astype(bf16)

    def tp_copy(source, target):
        return pltpu.make_async_remote_copy(
            src_ref=tp_ref.at[source],
            dst_ref=tp_ref.at[source],
            send_sem=tp_send.at[0],
            recv_sem=tp_recv.at[0],
            device_id={"tp": target},
            device_id_type=MESH,
        )

    def tp_all():
        some = tp_ref.at[pl.ds(0, n_tp - 1)]
        return pltpu.make_async_remote_copy(
            src_ref=some,
            dst_ref=some,
            send_sem=tp_send.at[0],
            recv_sem=tp_recv.at[0],
            device_id={"tp": flip(my_tp, 1, n_tp)},
            device_id_type=MESH,
        )

    for step in (2, 3, 1) if n_tp == 4 else reversed(range(1, n_tp)):
        tp_copy(my_tp, flip(my_tp, step, n_tp)).start()

    log_weight = peak + jnp.log(weight_sum) + cum_query
    for place in range(n_kv):
        order_ref[flip(me, place, n_kv), :, q_cols:] = log_weight[slot(place)]
    for owner in range(n_kv):
        fresh_ref[slot(owner), k_pad:] = order_ref[owner, :, q_cols:]
    log_ref[...] = jnp.transpose(fresh_ref[:, k_pad:])[:heads]

    rs1_all().wait_send()
    pltpu.make_async_remote_copy(
        src_ref=query_ref.at[everyone],
        dst_ref=query_ref.at[everyone],
        send_sem=ag1_send.at[0],
        recv_sem=ag1_recv.at[0],
        device_id={"kv": flip(me, 1, n_kv)},
        device_id_type=MESH,
    ).wait_send()
    new_all().wait_send()
    part_all(n_kv, 0).wait_send()
    tp_all().wait_recv()
    mixed = tp_ref[0].astype(f32)
    for source in range(1, n_tp):
        mixed = mixed + tp_ref[source].astype(f32)
    mixed_ref[...] = mixed.astype(bf16)
    tp_all().wait_send()


def shards(
    tokens,
    norm_gain,
    w_query,
    w_key,
    w_value,
    forget_weight,
    forget_bias,
    kv_cache,
    cum_gates,
    lengths,
    w_out,
):
    n_kv, n_tp = lax.axis_size("kv"), lax.axis_size("tp")
    rows, cols = tokens.shape
    span, kv_local, entry = kv_cache.shape[1:]
    heads = cum_gates.shape[1]
    q_cols, k_cols = w_query.shape[1], w_key.shape[1]
    k_pad = -(-k_cols // LANES) * LANES
    wide = q_cols + 2 * k_pad + LANES
    mine = rows // n_kv
    out_cols = w_out.shape[1]
    f32, bf16 = jnp.float32, jnp.bfloat16
    vmem = pl.BlockSpec(memory_space=pltpu.VMEM)
    hbm = pl.BlockSpec(memory_space=pl.ANY)
    dma = pltpu.SemaphoreType.DMA
    tall = (mine * heads, LANES)
    mixed, log_weight = pl.pallas_call(
        functools.partial(kernel, n_kv, n_tp),
        out_shape=(
            pltpu.VMEM((rows, out_cols), bf16),
            pltpu.VMEM((heads, rows), f32),
        ),
        in_specs=[hbm] * 11,
        out_specs=(vmem, vmem),
        scratch_shapes=[
            pltpu.VMEM(tokens.shape, bf16),
            pltpu.VMEM((1, cols), f32),
            pltpu.VMEM((1, heads), f32),
            pltpu.SMEM(lengths.shape, jnp.int32),
            pltpu.VMEM(w_query.shape, bf16),
            pltpu.VMEM(w_key.shape, bf16),
            pltpu.VMEM(w_value.shape, bf16),
            pltpu.VMEM((LANES, cols), bf16),
            pltpu.VMEM((rows, span * kv_local, entry), bf16),
            pltpu.VMEM(cum_gates.shape, f32),
            pltpu.VMEM(w_out.shape, bf16),
            pltpu.VMEM((3, mine * (entry // 2), span * kv_local), bf16),
            pltpu.VMEM((rows, heads, span * kv_local), f32),
            pltpu.VMEM((rows, heads, LANES), f32),
            pltpu.VMEM((n_kv, mine, wide), bf16),
            pltpu.VMEM((n_kv, mine, wide), bf16),
            pltpu.VMEM((n_kv, mine, q_cols), bf16),
            pltpu.VMEM((n_kv, mine, k_pad + LANES), f32),
            pltpu.VMEM((1, LANES), f32),
            pltpu.VMEM(tall, f32),
            pltpu.VMEM((2, mine // 2, 2 * heads, span * kv_local), f32),
            pltpu.VMEM((2, mine // 2, 2 * heads, LANES), f32),
            pltpu.VMEM(tall, f32),
            pltpu.VMEM(tall, f32),
            pltpu.VMEM((n_kv, n_kv, mine, q_cols + LANES), bf16),
            pltpu.VMEM((n_kv, rows, q_cols + LANES), f32),
            pltpu.VMEM((rows, k_pad + LANES), f32),
            pltpu.VMEM((n_kv, mine, q_cols + LANES), f32),
            pltpu.VMEM((rows, q_cols), f32),
            pltpu.VMEM((n_tp, rows, out_cols), bf16),
            dma((10,)),
            dma((n_kv,)),
            dma((1,)),
            dma((1,)),
            dma((1,)),
            dma((n_kv,)),
            dma((1,)),
            dma((1,)),
            dma((1,)),
            dma((2,)),
            dma((1,)),
            dma((1,)),
        ],
        compiler_params=pltpu.CompilerParams(
            collective_id=0, has_side_effects=True, vmem_limit_bytes=56 * 1024 * 1024
        ),
    )(
        tokens,
        norm_gain.reshape(1, cols),
        forget_bias.reshape(1, heads),
        lengths,
        w_query,
        w_key,
        w_value,
        forget_weight.T,
        kv_cache.reshape(rows, span * kv_local, entry),
        cum_gates,
        w_out,
    )
    return mixed, log_weight.T


def solution(mesh):
    placed = (
        P(None, "kv"),
        P("kv"),
        P("kv", "tp"),
        P("kv", "tp"),
        P("kv", "tp"),
        P(),
        P("tp"),
        P(None, "kv", "tp", None),
        P(None, "tp", "kv"),
        P(),
        P("tp", "kv"),
    )
    return jax.shard_map(
        shards,
        mesh=mesh,
        in_specs=placed,
        out_specs=(P(None, "kv"), P(None, "tp")),
        check_vma=False,
    )
```

```python
import functools
import jax
import jax.numpy as jnp
from jax import lax
from jax.experimental import pallas as pl
from jax.experimental.pallas import tpu as pltpu
from jax.sharding import PartitionSpec as P

norm_eps = 1e-05
masked_floor = -1e30
LANES = 128
MESH = pl.DeviceIdType.MESH


def flip(index, step, count):
    out = index
    bit = 1
    while bit < count:
        out = out + bit * ((step // bit) % 2) * (1 - 2 * ((index // bit) % 2))
        bit *= 2
    return out


def lane_of(shape):
    return lax.broadcasted_iota(jnp.int32, shape, len(shape) - 1)


def kernel(
    n_kv,
    n_tp,
    tokens_hbm,
    gain_hbm,
    bias_hbm,
    lengths_hbm,
    w_query_hbm,
    w_key_hbm,
    w_value_hbm,
    gate_hbm,
    cache_hbm,
    cum_hbm,
    w_out_hbm,
    mixed_ref,
    log_ref,
    tokens_ref,
    gain_ref,
    bias_ref,
    lengths_ref,
    w_query_ref,
    w_key_ref,
    w_value_ref,
    gate_ref,
    cache_ref,
    cum_ref,
    w_out_ref,
    turned_ref,
    shift_ref,
    last_ref,
    proj_ref,
    rs1_ref,
    query_ref,
    new_ref,
    bias_pad_ref,
    wide_ref,
    score_ref,
    peak_ref,
    value_ref,
    stat_ref,
    part_ref,
    gathered_ref,
    fresh_ref,
    order_ref,
    wide_rows_ref,
    tp_ref,
    weight_sems,
    cache_sems,
    rs1_send,
    rs1_recv,
    ag1_send,
    ag1_recv,
    new_send,
    new_recv,
    part_send,
    part_recv,
    tp_send,
    tp_recv,
):
    f32, bf16 = jnp.float32, jnp.bfloat16
    me = lax.axis_index("kv")
    my_tp = lax.axis_index("tp")
    rows, cols = tokens_ref.shape
    heads = cum_ref.shape[1]
    span = cum_ref.shape[2]
    entries = cache_ref.shape[1]
    kv_local = entries // span
    group = heads // kv_local
    head_size = LANES // 2
    all_heads = gate_hbm.shape[0]
    mine = rows // n_kv
    pairs = mine // 2
    q_cols = w_query_ref.shape[1]
    k_cols = w_key_ref.shape[1]
    k_pad = -(-k_cols // LANES) * LANES
    model_width = cols * n_kv
    inv_root = head_size ** (-0.5)
    chunk_cols = 2 * LANES
    chunks = range(0, entries, chunk_cols)
    segment = LANES // 4

    offset = pl.multiple_of(me * cols, cols)
    loads = [
        pltpu.make_async_copy(src, dst, weight_sems.at[i])
        for i, (src, dst) in enumerate(
            [
                (tokens_hbm, tokens_ref),
                (gain_hbm, gain_ref),
                (w_query_hbm, w_query_ref),
                (w_key_hbm, w_key_ref),
                (w_value_hbm, w_value_ref),
                (gate_hbm.at[:, pl.ds(offset, cols)], gate_ref.at[pl.ds(0, all_heads)]),
                (bias_hbm, bias_ref),
                (lengths_hbm, lengths_ref),
                (cum_hbm, cum_ref),
                (w_out_hbm, w_out_ref),
            ]
        )
    ]
    barrier = pltpu.get_barrier_semaphore()
    for step in range(1, n_kv):
        pl.semaphore_signal(
            barrier, inc=1, device_id={"kv": flip(me, step, n_kv)}, device_id_type=MESH
        )
    for step in range(1, n_tp):
        pl.semaphore_signal(
            barrier, inc=1, device_id={"tp": flip(my_tp, step, n_tp)}, device_id_type=MESH
        )
    for load in loads[:9]:
        load.start()

    def cache_load(owner):
        at = pl.ds(owner * mine, mine)
        return pltpu.make_async_copy(cache_hbm.at[at], cache_ref.at[at], cache_sems.at[owner])

    gate_ref[all_heads:, :] = jnp.zeros((LANES - all_heads, cols), bf16)
    bias_pad_ref[...] = jnp.zeros_like(bias_pad_ref)
    for load in loads[:2]:
        load.wait()
    tokens_f = tokens_ref[...].astype(f32)
    squares = jnp.sum(tokens_f * tokens_f, axis=1, keepdims=True)
    normed = (tokens_f * gain_ref[...]).astype(bf16)
    for load in loads[2:8]:
        load.wait()
    ahead = turned_ref.shape[0]
    flight = 3
    for step in range(1, flight + 1):
        cache_load(flip(me, step, n_kv)).start()
    loads[9].start()
    bias_pad_ref[:, 0:heads] = bias_ref[...]
    pieces = [jnp.dot(normed, w_query_ref[...], preferred_element_type=f32)]
    for w_ref in (w_key_ref, w_value_ref):
        piece = jnp.dot(normed, w_ref[...], preferred_element_type=f32)
        if k_pad > k_cols:
            piece = jnp.concatenate([piece, jnp.zeros((rows, k_pad - k_cols), f32)], axis=1)
        pieces.append(piece)
    gates = lax.dot_general(
        normed, gate_ref[...], (((1,), (1,)), ((), ())), preferred_element_type=f32
    )
    pieces.append(jnp.where(lane_of(gates.shape) == all_heads, squares, gates))
    at = 0
    for piece in pieces:
        for owner in range(n_kv):
            proj_ref[owner, :, at : at + piece.shape[1]] = piece[
                owner * mine : (owner + 1) * mine
            ].astype(bf16)
        at += piece.shape[1]

    everyone = pl.ds(0, n_kv - 1)

    def rs1_copy(source, target):
        return pltpu.make_async_remote_copy(
            src_ref=proj_ref.at[target],
            dst_ref=rs1_ref.at[source],
            send_sem=rs1_send.at[0],
            recv_sem=rs1_recv.at[0],
            device_id={"kv": target},
            device_id_type=MESH,
        )

    def rs1_all():
        return pltpu.make_async_remote_copy(
            src_ref=proj_ref.at[everyone],
            dst_ref=rs1_ref.at[everyone],
            send_sem=rs1_send.at[0],
            recv_sem=rs1_recv.at[0],
            device_id={"kv": flip(me, 1, n_kv)},
            device_id_type=MESH,
        )

    loads[8].wait()
    tile = (heads, LANES)
    lane = lane_of(tile)
    own_column = (lane % kv_local) == (lax.broadcasted_iota(jnp.int32, tile, 0) // group)

    def prepare(row):
        length = lengths_ref[row] - me * span
        last = jnp.zeros(tile, f32)
        for chunk in range(span // LANES):
            cum = cum_ref[row, :, chunk * LANES : (chunk + 1) * LANES]
            place = lane + chunk * LANES
            shift = jnp.where(place < length, -cum, masked_floor)
            last = last + jnp.where(place == length - 1, cum, 0.0)
            for part in range(kv_local):
                if kv_local == 1:
                    spread = shift
                else:
                    pick = lane // kv_local + part * (LANES // kv_local)
                    spread = jnp.take_along_axis(shift, pick, axis=1)
                    spread = jnp.where(own_column, spread, masked_floor)
                at = (chunk * kv_local + part) * LANES
                shift_ref[row, :, at : at + LANES] = spread
        last_ref[row] = jnp.broadcast_to(jnp.sum(last, axis=1, keepdims=True), tile)

    def prepare_block(step, carry):
        owner = flip(me, step, n_kv)
        for i in range(mine):
            prepare(owner * mine + i)
        return carry

    def cached(row_a, row_b, at):
        inside = slice(at, at + chunk_cols)
        return jnp.concatenate([cache_ref[row_a, inside, :], cache_ref[row_b, inside, :]], axis=1)

    pick_shape = (LANES, 2 * LANES)
    pick_row = lax.broadcasted_iota(jnp.int32, pick_shape, 0)
    pick = (
        lane_of(pick_shape) == pick_row + (pick_row // head_size) * head_size
    ).astype(f32).astype(bf16)

    def following(step):
        place = step + flight
        past = place // (ahead + 1)
        beyond = place // (ahead + 2)
        return place - past * (ahead + 1) + beyond * (ahead + 1) - beyond

    def turn(step, carry):
        owner = flip(me, step, n_kv)
        cache_load(owner).wait()
        cache_load(flip(me, following(step), n_kv)).start()
        for pair in range(pairs):
            row = owner * mine + 2 * pair
            for at in chunks:
                turned_ref[step - 1, pair * LANES : (pair + 1) * LANES, at : at + chunk_cols] = (
                    lax.dot_general(
                        pick,
                        cached(row, row + 1, at),
                        (((1,), (1,)), ((), ())),
                        preferred_element_type=f32,
                    ).astype(bf16)
                )
        return carry

    few = n_kv - n_kv // 8
    ready_blocks = 3 * ((n_kv + n_kv // 2 - 1 - me) // few)
    turned_blocks = 1 + (n_kv - 1 - me) // few + (n_kv + n_kv // 4 - 1 - me) // few
    lax.fori_loop(0, ready_blocks, prepare_block, 0)
    lax.fori_loop(1, turned_blocks, turn, 0)
    pl.semaphore_wait(barrier, n_kv + n_tp - 2)
    for step in reversed(range(1, n_kv)):
        rs1_copy(me, flip(me, step, n_kv)).start()
    lax.fori_loop(ready_blocks, 3, prepare_block, 0)
    lax.fori_loop(turned_blocks, ahead + 1, turn, 0)
    for place in range(ahead + flight + 1, n_kv + 1):
        cache_load(flip(me, place - 1, n_kv)).start()

    total = proj_ref[me].astype(f32)
    rs1_all().wait_recv()
    for step in range(1, n_kv):
        total = total + rs1_ref[flip(me, step, n_kv)].astype(f32)
    misc = total[:, q_cols + 2 * k_pad :]
    part_lane = lane_of((mine, LANES))
    total_sq = jnp.sum(jnp.where(part_lane == all_heads, misc, 0.0), axis=1, keepdims=True)
    row_scale = lax.rsqrt(total_sq / model_width + norm_eps)
    query_ref[me] = (row_scale * total[:, :q_cols]).astype(bf16)

    def ag1_copy(source, target):
        return pltpu.make_async_remote_copy(
            src_ref=query_ref.at[source],
            dst_ref=query_ref.at[source],
            send_sem=ag1_send.at[0],
            recv_sem=ag1_recv.at[source],
            device_id={"kv": target},
            device_id_type=MESH,
        )

    for step in reversed(range(1, n_kv)):
        ag1_copy(me, flip(me, step, n_kv)).start()

    low_half = part_lane < head_size
    even_row = lax.broadcasted_iota(jnp.int32, (mine, LANES), 0) % 2 == 0

    def grouped(values, width):
        tiles = []
        for at in range(0, width, LANES):
            halves = []
            for half in range(2):
                source = (at // head_size + half) // group
                found = values[:, (source // 2) * LANES : (source // 2 + 1) * LANES]
                if source % 2 != half:
                    found = pltpu.roll(found, head_size, 1)
                halves.append(found)
            low = lane_of(halves[0].shape) < head_size
            tiles.append(jnp.where(low, halves[0], halves[1]))
        return jnp.concatenate(tiles, axis=1)

    head_shape = (LANES, q_cols)
    head_map = (
        lax.broadcasted_iota(jnp.int32, head_shape, 0) % heads
        == lax.broadcasted_iota(jnp.int32, head_shape, 1) // head_size
    ).astype(f32).astype(bf16)

    new_key = (row_scale * total[:, q_cols : q_cols + k_pad]).astype(bf16).astype(f32)
    new_value = (row_scale * total[:, q_cols + k_pad : q_cols + 2 * k_pad]).astype(bf16)
    product = query_ref[me].astype(f32) * grouped(new_key, q_cols)
    coarse = product.astype(bf16)
    fine = (product - coarse.astype(f32)).astype(bf16)
    new_score = sum(
        lax.dot_general(part, head_map, (((1,), (1,)), ((), ())), preferred_element_type=f32)
        for part in (coarse, fine)
    )
    gate = pltpu.roll(row_scale * misc, (LANES - my_tp * heads) % LANES, 1) + bias_pad_ref[...]
    log_gate = jnp.minimum(gate, 0.0) - jnp.log1p(jnp.exp(-jnp.abs(gate)))
    new_ref[me, :, :k_pad] = new_value.astype(f32)
    new_ref[me, :, k_pad:] = jnp.where(
        part_lane < heads, new_score * inv_root, pltpu.roll(log_gate, heads, 1)
    )

    def new_copy(source, target):
        return pltpu.make_async_remote_copy(
            src_ref=new_ref.at[source],
            dst_ref=new_ref.at[source],
            send_sem=new_send.at[0],
            recv_sem=new_recv.at[0],
            device_id={"kv": target},
            device_id_type=MESH,
        )

    def new_all():
        return pltpu.make_async_remote_copy(
            src_ref=new_ref.at[everyone],
            dst_ref=new_ref.at[everyone],
            send_sem=new_send.at[0],
            recv_sem=new_recv.at[0],
            device_id={"kv": flip(me, 1, n_kv)},
            device_id_type=MESH,
        )

    for step in reversed(range(1, n_kv)):
        new_copy(me, flip(me, step, n_kv)).start()

    early = n_kv - 2

    def part_copy(source, block, target, stage):
        return pltpu.make_async_remote_copy(
            src_ref=part_ref.at[source, block],
            dst_ref=part_ref.at[source, block],
            send_sem=part_send.at[0],
            recv_sem=part_recv.at[stage],
            device_id={"kv": target},
            device_id_type=MESH,
        )

    def part_all(count, stage):
        some = part_ref.at[pl.ds(0, count), everyone]
        return pltpu.make_async_remote_copy(
            src_ref=some,
            dst_ref=some,
            send_sem=part_send.at[0],
            recv_sem=part_recv.at[stage],
            device_id={"kv": flip(me, 1, n_kv)},
            device_id_type=MESH,
        )

    zeros = jnp.zeros((heads, LANES), f32)
    tall_pair = lax.broadcasted_iota(jnp.int32, (mine * heads, LANES), 0) // (2 * heads)
    stat_kind = (lane % segment) // heads

    def weigh(pair, buffer):
        peak = peak_ref[buffer, pair, :, :1]
        sums = jnp.zeros((2 * heads, chunk_cols), f32)
        weights = []
        for at in chunks:
            weight = jnp.exp(score_ref[buffer, pair, :, at : at + chunk_cols] - peak)
            sums = sums + weight
            weights.append(weight.astype(bf16))
        return weights, jnp.sum(sums, axis=1, keepdims=True), peak

    def shifts(row, count, at):
        return jnp.concatenate(
            [shift_ref[row + i, :, at : at + chunk_cols] for i in range(count)], axis=0
        )

    def score(owner, pair, buffer):
        first, second = 2 * pair, 2 * pair + 1
        row_a, row_b = owner * mine + first, owner * mine + second
        left = wide_ref[first * heads : (first + 1) * heads, :]
        right = wide_ref[second * heads : (second + 1) * heads, :]
        queries = jnp.concatenate(
            [
                jnp.concatenate([left, zeros], axis=1),
                jnp.concatenate([zeros, right], axis=1),
            ],
            axis=0,
        ).astype(bf16)
        peak = None
        for at in chunks:
            part = lax.dot_general(
                queries,
                cached(row_a, row_b, at),
                (((1,), (1,)), ((), ())),
                preferred_element_type=f32,
            )
            part = part + shifts(row_a, 2, at)
            score_ref[buffer, pair, :, at : at + chunk_cols] = part
            peak = part if peak is None else jnp.maximum(peak, part)
        peak_ref[buffer, pair] = jnp.broadcast_to(
            jnp.max(peak, axis=1, keepdims=True), (2 * heads, LANES)
        )

    def score_turned(step, buffer):
        owner = flip(me, step, n_kv)
        query = query_ref[owner].astype(f32) * inv_root
        for head in range(heads):
            at = (head // 2) * LANES
            found = query[:, at : at + LANES]
            other = pltpu.roll(found, head_size, 1)
            low, high = (found, other) if head % 2 == 0 else (other, found)
            wide_ref[pl.ds(head, mine, stride=heads), :] = jnp.where(
                even_row, jnp.where(low_half, low, 0.0), jnp.where(low_half, 0.0, high)
            )
        wide = wide_ref[...]
        queries = jnp.concatenate(
            [jnp.where(tall_pair == pair, wide, 0.0) for pair in range(pairs)], axis=1
        ).astype(bf16)
        peak = None
        for at in chunks:
            part = jnp.dot(
                queries,
                turned_ref[step - 1, :, at : at + chunk_cols],
                preferred_element_type=f32,
            )
            part = part + shifts(owner * mine, mine, at)
            for pair in range(pairs):
                score_ref[buffer, pair, :, at : at + chunk_cols] = part[
                    pair * 2 * heads : (pair + 1) * 2 * heads
                ]
            peak = part if peak is None else jnp.maximum(peak, part)
        peak = jnp.broadcast_to(jnp.max(peak, axis=1, keepdims=True), (mine * heads, LANES))
        for pair in range(pairs):
            peak_ref[buffer, pair] = peak[pair * 2 * heads : (pair + 1) * 2 * heads]

    def gather(owner, pair, weights, total_weight, peak):
        first, second = 2 * pair, 2 * pair + 1
        row_a, row_b = owner * mine + first, owner * mine + second
        values = jnp.zeros((2 * heads, chunk_cols), f32)
        for weight, at in zip(weights, chunks):
            values = values + jnp.dot(
                weight, cached(row_a, row_b, at), preferred_element_type=f32
            )
        for i, (place, row) in enumerate(((first, row_a), (second, row_b))):
            inside = slice(i * heads, (i + 1) * heads)
            place_rows = slice(place * heads, (place + 1) * heads)
            value_ref[place_rows, :] = values[inside, i * LANES : (i + 1) * LANES]
            stat_ref[place_rows, :] = jnp.where(
                stat_kind == 0,
                peak[inside],
                jnp.where(stat_kind == 1, total_weight[inside], last_ref[row]),
            )

    def ready(owner):
        query = query_ref[owner].astype(f32) * inv_root
        for head in range(heads):
            at = (head // 2) * LANES
            found = query[:, at : at + LANES]
            if head % 2 == 1:
                found = pltpu.roll(found, head_size, 1)
            wide_ref[pl.ds(head, mine, stride=heads), :] = jnp.where(low_half, found, 0.0)

    def send(owner, stage):
        stats = jnp.zeros((mine, LANES), f32)
        held = None
        for head in range(heads):
            inside = pl.ds(head, mine, stride=heads)
            stats = jnp.where(part_lane % heads == head, stat_ref[inside, :], stats)
            found = value_ref[inside, :]
            if head % 2 == 0:
                held = pltpu.roll(found, head_size, 1)
            else:
                at = (head // 2) * LANES
                part_ref[me, owner, :, at : at + LANES] = jnp.where(low_half, held, found).astype(
                    bf16
                )
        coarse = stats.astype(bf16).astype(f32)
        medium = (stats - coarse).astype(bf16).astype(f32)
        fine = stats - coarse - medium
        part_ref[me, owner, :, q_cols:] = jnp.where(
            part_lane < segment, coarse, jnp.where(part_lane < 2 * segment, medium, fine)
        ).astype(bf16)
        for step in reversed(range(1, n_kv)):
            part_copy(me, owner, flip(me, step, n_kv), stage).start()

    cache_load(me).wait()
    ready(me)
    for pair in range(pairs):
        score(me, pair, 0)
    for pair in range(pairs):
        gather(me, pair, *weigh(pair, 0))
    send(me, 0)
    ag1_copy(flip(me, 1, n_kv), me).wait_recv()
    score_turned(1, 0)
    for step in range(1, ahead):
        ag1_copy(flip(me, step + 1, n_kv), me).wait_recv()
        owner = flip(me, step, n_kv)
        now, later = (step - 1) % 2, step % 2
        prepare_block(step + 2, 0)
        score_turned(step + 1, later)
        for pair in range(pairs):
            gather(owner, pair, *weigh(pair, now))
        send(owner, 0)
    last_buffer = (ahead - 1) % 2

    def attend(step, carry):
        owner, after = flip(me, step, n_kv), flip(me, step + 1, n_kv)
        cache_load(after).wait()
        ag1_copy(after, me).wait_recv()
        prepare_block(step + 2, 0)
        ready(after)
        for pair in range(pairs):
            weights = weigh(pair, last_buffer)
            score(after, pair, last_buffer)
            gather(owner, pair, *weights)
        send(owner, step // early)
        return carry

    lax.fori_loop(ahead, n_kv - 1, attend, 0)
    final = flip(me, n_kv - 1, n_kv)
    for pair in range(pairs):
        gather(final, pair, *weigh(pair, last_buffer))
    send(final, 1)

    def slot(place):
        return slice(place * mine, (place + 1) * mine)

    new_all().wait_recv()
    for place in range(n_kv):
        fresh_ref[slot(place), :] = new_ref[flip(me, place, n_kv)]
    loads[9].wait()
    row_lane = lane_of((rows, LANES))
    fresh = fresh_ref[:, k_pad:]
    fresh_gate = pltpu.roll(fresh, LANES - heads, 1)
    fresh_values = grouped(fresh_ref[:, :k_pad], q_cols)
    merge_shape = (LANES, 3 * LANES)
    merge_row = lax.broadcasted_iota(jnp.int32, merge_shape, 0)
    merge_place = merge_row % segment
    merge_lane = lane_of(merge_shape)
    merge_map = (
        (merge_row < 3 * segment)
        & (merge_place // heads == merge_lane // LANES)
        & (merge_place % heads == merge_lane % LANES)
    ).astype(f32).astype(bf16)
    scale_map = jnp.concatenate([head_map, head_map], axis=0)
    for step in range(n_kv):
        if step == 0:
            part_all(early, 0).wait_recv()
        if step == early:
            part_all(n_kv - early, 1).wait_recv()
        for place in range(n_kv):
            source = flip(me, place, n_kv)
            block = flip(me, place ^ step, n_kv)
            gathered_ref[place, slot(place ^ step), :] = part_ref[source, block].astype(f32)

    merged = jnp.dot(
        jnp.concatenate(
            [gathered_ref[place, :, q_cols:].astype(bf16) for place in range(n_kv)], axis=0
        ),
        merge_map,
        preferred_element_type=f32,
    )

    def stat(place, kind):
        return merged[place * rows : (place + 1) * rows, kind * LANES : (kind + 1) * LANES]

    cum_query = fresh_gate
    for place in range(n_kv):
        cum_query = cum_query + stat(place, 2)
    new_biased = fresh - cum_query
    peak = new_biased
    for place in range(n_kv):
        peak = jnp.maximum(peak, stat(place, 0))
    new_weight = jnp.exp(new_biased - peak)
    weight_sum = new_weight
    factors = []
    for place in range(n_kv):
        factor = jnp.exp(stat(place, 0) - peak)
        weight_sum = weight_sum + factor * stat(place, 1)
        factors.append(factor)
    factors.append(new_weight.astype(bf16).astype(f32))
    inverse = jnp.where(row_lane < heads, 1.0 / weight_sum, 0.0)
    scales = []
    for factor in factors:
        scale = jnp.where(row_lane < heads, factor * inverse, 0.0)
        coarse = scale.astype(bf16)
        fine = (scale - coarse.astype(f32)).astype(bf16)
        scales.append(jnp.concatenate([coarse, fine], axis=1))
    wide = jnp.dot(jnp.concatenate(scales, axis=0), scale_map, preferred_element_type=f32)
    attended = wide[n_kv * rows :] * fresh_values
    for place in range(n_kv):
        attended = attended + wide[place * rows : (place + 1) * rows] * (
            gathered_ref[place, :, :q_cols]
        )
    for place in range(n_kv):
        order_ref[flip(me, place, n_kv), :, :q_cols] = attended[slot(place)]
    for owner in range(n_kv):
        wide_rows_ref[slot(owner), :] = order_ref[owner, :, :q_cols]
    tp_ref[my_tp] = jnp.dot(
        wide_rows_ref[...].astype(bf16), w_out_ref[...], preferred_element_type=f32
    ).astype(bf16)

    def tp_copy(source, target):
        return pltpu.make_async_remote_copy(
            src_ref=tp_ref.at[source],
            dst_ref=tp_ref.at[source],
            send_sem=tp_send.at[0],
            recv_sem=tp_recv.at[0],
            device_id={"tp": target},
            device_id_type=MESH,
        )

    def tp_all():
        some = tp_ref.at[pl.ds(0, n_tp - 1)]
        return pltpu.make_async_remote_copy(
            src_ref=some,
            dst_ref=some,
            send_sem=tp_send.at[0],
            recv_sem=tp_recv.at[0],
            device_id={"tp": flip(my_tp, 1, n_tp)},
            device_id_type=MESH,
        )

    for step in (2, 3, 1) if n_tp == 4 else reversed(range(1, n_tp)):
        tp_copy(my_tp, flip(my_tp, step, n_tp)).start()

    log_weight = peak + jnp.log(weight_sum) + cum_query
    for place in range(n_kv):
        order_ref[flip(me, place, n_kv), :, q_cols:] = log_weight[slot(place)]
    for owner in range(n_kv):
        fresh_ref[slot(owner), k_pad:] = order_ref[owner, :, q_cols:]
    log_ref[...] = jnp.transpose(fresh_ref[:, k_pad:])[:heads]

    rs1_all().wait_send()
    pltpu.make_async_remote_copy(
        src_ref=query_ref.at[everyone],
        dst_ref=query_ref.at[everyone],
        send_sem=ag1_send.at[0],
        recv_sem=ag1_recv.at[0],
        device_id={"kv": flip(me, 1, n_kv)},
        device_id_type=MESH,
    ).wait_send()
    new_all().wait_send()
    part_all(n_kv, 0).wait_send()
    tp_all().wait_recv()
    mixed = tp_ref[0].astype(f32)
    for source in range(1, n_tp):
        mixed = mixed + tp_ref[source].astype(f32)
    mixed_ref[...] = mixed.astype(bf16)
    tp_all().wait_send()


def shards(
    tokens,
    norm_gain,
    w_query,
    w_key,
    w_value,
    forget_weight,
    forget_bias,
    kv_cache,
    cum_gates,
    lengths,
    w_out,
):
    n_kv, n_tp = lax.axis_size("kv"), lax.axis_size("tp")
    rows, cols = tokens.shape
    span, kv_local, entry = kv_cache.shape[1:]
    heads = cum_gates.shape[1]
    q_cols, k_cols = w_query.shape[1], w_key.shape[1]
    k_pad = -(-k_cols // LANES) * LANES
    wide = q_cols + 2 * k_pad + LANES
    mine = rows // n_kv
    out_cols = w_out.shape[1]
    f32, bf16 = jnp.float32, jnp.bfloat16
    vmem = pl.BlockSpec(memory_space=pltpu.VMEM)
    hbm = pl.BlockSpec(memory_space=pl.ANY)
    dma = pltpu.SemaphoreType.DMA
    tall = (mine * heads, LANES)
    mixed, log_weight = pl.pallas_call(
        functools.partial(kernel, n_kv, n_tp),
        out_shape=(
            pltpu.VMEM((rows, out_cols), bf16),
            pltpu.VMEM((heads, rows), f32),
        ),
        in_specs=[hbm] * 11,
        out_specs=(vmem, vmem),
        scratch_shapes=[
            pltpu.VMEM(tokens.shape, bf16),
            pltpu.VMEM((1, cols), f32),
            pltpu.VMEM((1, heads), f32),
            pltpu.SMEM(lengths.shape, jnp.int32),
            pltpu.VMEM(w_query.shape, bf16),
            pltpu.VMEM(w_key.shape, bf16),
            pltpu.VMEM(w_value.shape, bf16),
            pltpu.VMEM((LANES, cols), bf16),
            pltpu.VMEM((rows, span * kv_local, entry), bf16),
            pltpu.VMEM(cum_gates.shape, f32),
            pltpu.VMEM(w_out.shape, bf16),
            pltpu.VMEM((4, mine * (entry // 2), span * kv_local), bf16),
            pltpu.VMEM((rows, heads, span * kv_local), f32),
            pltpu.VMEM((rows, heads, LANES), f32),
            pltpu.VMEM((n_kv, mine, wide), bf16),
            pltpu.VMEM((n_kv, mine, wide), bf16),
            pltpu.VMEM((n_kv, mine, q_cols), bf16),
            pltpu.VMEM((n_kv, mine, k_pad + LANES), f32),
            pltpu.VMEM((1, LANES), f32),
            pltpu.VMEM(tall, f32),
            pltpu.VMEM((2, mine // 2, 2 * heads, span * kv_local), f32),
            pltpu.VMEM((2, mine // 2, 2 * heads, LANES), f32),
            pltpu.VMEM(tall, f32),
            pltpu.VMEM(tall, f32),
            pltpu.VMEM((n_kv, n_kv, mine, q_cols + LANES), bf16),
            pltpu.VMEM((n_kv, rows, q_cols + LANES), f32),
            pltpu.VMEM((rows, k_pad + LANES), f32),
            pltpu.VMEM((n_kv, mine, q_cols + LANES), f32),
            pltpu.VMEM((rows, q_cols), f32),
            pltpu.VMEM((n_tp, rows, out_cols), bf16),
            dma((10,)),
            dma((n_kv,)),
            dma((1,)),
            dma((1,)),
            dma((1,)),
            dma((n_kv,)),
            dma((1,)),
            dma((1,)),
            dma((1,)),
            dma((2,)),
            dma((1,)),
            dma((1,)),
        ],
        compiler_params=pltpu.CompilerParams(
            collective_id=0, has_side_effects=True, vmem_limit_bytes=56 * 1024 * 1024
        ),
    )(
        tokens,
        norm_gain.reshape(1, cols),
        forget_bias.reshape(1, heads),
        lengths,
        w_query,
        w_key,
        w_value,
        forget_weight.T,
        kv_cache.reshape(rows, span * kv_local, entry),
        cum_gates,
        w_out,
    )
    return mixed, log_weight.T


def solution(mesh):
    placed = (
        P(None, "kv"),
        P("kv"),
        P("kv", "tp"),
        P("kv", "tp"),
        P("kv", "tp"),
        P(),
        P("tp"),
        P(None, "kv", "tp", None),
        P(None, "tp", "kv"),
        P(),
        P("tp", "kv"),
    )
    return jax.shard_map(
        shards,
        mesh=mesh,
        in_specs=placed,
        out_specs=(P(None, "kv"), P(None, "tp")),
        check_vma=False,
    )
```
